256 devices in a mesh: row: 32 (over z, y), col: 8 (over x, core).
Axes of the slice: x: 4, y: 4, z: 8, core: 2. Of those that a mesh axis runs over, the one named last changes fastest.
Arguments:
- tokens: bfloat16 [2, 65536, 1024], P(None, 'row'), may hold values from -6 to 6
- norm_gain: float32 [1024], replicated, may hold values from 0.1 to 1.9
- w_fourier_in: bfloat16 [1024, 512], P(None, 'col'), may hold values from -0.1875 to 0.1875
- w_gate: bfloat16 [1024, 1024], replicated, may hold values from -0.1875 to 0.1875
- w_spectrum: bfloat16 [512, 1024], replicated, may hold values from -0.25 to 0.25
- w_output: bfloat16 [1024, 1024], P(None, 'col'), may hold values from -0.375 to 0.375
Outputs:
- block_output: bfloat16 [2, 65536, 1024], P(None, 'row', 'col')
The draws below stay inside these ranges and needn't reach their ends.
All inputs are finite; a program needn't handle non-finite values.
Results may differ from the reference program's by a relative error of at most 0.015.
Values may be sent and summed in bfloat16 or wider, within the bound.
A program may use at most 320 MiB of HBM per device.

```python
import jax
import jax.numpy as jnp
from jax import lax

D = 1024
GROUPS = 8
GROUP_WIDTH = 64
FOURIER_WIDTH = 512
SEQS = 2
SEQ = 65536


def block_scale(stream_key, dims, cuts, low, largest):
    gain, own = 1.0, jax.random.fold_in(stream_key, 6)
    for axis_at, parts in cuts:
        steps = jnp.exp(jax.random.uniform(jax.random.fold_in(own, axis_at), (parts,), jnp.float32, low / len(cuts), largest / len(cuts)))
        gain = gain * jnp.repeat(steps, dims[axis_at] // parts).reshape([-1 if axis == axis_at else 1 for axis in range(len(dims))])
    return gain


def normal_values(own_key, dims, spread, bound, split=(), held_as=jnp.bfloat16):
    values = jax.random.normal(own_key, dims, jnp.float32) * spread
    if len(split) > 0:
        values = block_scale(own_key, dims, split, -0.22, 0.18) * values
    return jnp.clip(values, min=-bound, max=bound).astype(held_as)


def setup_inputs(seed: int = 0) -> dict:
    key_list = jax.random.split(jax.random.key(seed), 7)
    return {
        "tokens": normal_values(key_list[0], (SEQS, SEQ, D), 1.0, 6.0, ((1, 32),)),
        "norm_gain": jnp.clip(1.0 + 0.18 * jax.random.normal(key_list[1], (D,), jnp.float32), 0.1, 1.9),
        "w_fourier_in": normal_values(key_list[2], (D, FOURIER_WIDTH), D ** -0.5, 0.1875, ((1, 8),)),
        "w_gate": normal_values(key_list[3], (D, D), D ** -0.5, 0.1875),
        "w_spectrum": normal_values(key_list[4], (FOURIER_WIDTH, D), FOURIER_WIDTH ** -0.5, 0.25),
        "w_output": normal_values(key_list[5], (D, D), (D // 4) ** -0.5, 0.375, ((1, 8),)),
    }


norm_eps = 1e-6


def reference(tokens, norm_gain, w_fourier_in, w_gate, w_spectrum, w_output):
    widened = tokens.astype(jnp.float32)
    inverse = lax.rsqrt(jnp.mean(widened * widened, axis=-1, keepdims=True) + norm_eps)
    normed = (widened * inverse * norm_gain).astype(jnp.bfloat16).reshape(SEQS * SEQ, D)
    fourier_in = jnp.dot(normed, w_fourier_in, preferred_element_type=jnp.float32).astype(jnp.bfloat16)
    grouped = fourier_in.astype(jnp.float32).reshape(SEQS, SEQ, GROUPS, GROUP_WIDTH)
    spectrum = jnp.real(jnp.fft.fft2(grouped, axes=(1, 3), norm="ortho")).astype(jnp.bfloat16)
    spectrum = spectrum.reshape(SEQS * SEQ, FOURIER_WIDTH)
    mixed_pre = jnp.dot(spectrum, w_spectrum, preferred_element_type=jnp.float32).astype(jnp.bfloat16)
    gate_pre = jnp.dot(normed, w_gate, preferred_element_type=jnp.float32)
    mixed = (jax.nn.sigmoid(gate_pre) * mixed_pre.astype(jnp.float32)).astype(jnp.bfloat16)
    block_output = jnp.dot(mixed, w_output, preferred_element_type=jnp.float32).astype(jnp.bfloat16)
    return block_output.reshape(SEQS, SEQ, D)
```

```python
import functools

import jax
import jax.numpy as jnp
import numpy as np
from jax import lax
from jax.experimental import pallas as pl
from jax.experimental.pallas import tpu as pltpu
from jax.sharding import PartitionSpec as P

GROUP_WIDTH = 64
FIRST_LEN = 256
LANES = 128


norm_eps = 1e-06


def shortened(value):
    return jax.tree.map(lambda a: a.astype(jnp.bfloat16) if a.dtype == jnp.float32 else a, value)


def over_all(value, axis, dim, absorb, carry):
    whole = jax.tree.map(lambda part: lax.all_gather(part, axis, axis=dim, tiled=True), value)
    return absorb(carry, whole, jnp.int32(0))


def dft_tables(length_in, length_out, period):
    left_index = lax.broadcasted_iota(jnp.int32, (length_in, length_out), 0)
    right_index = lax.broadcasted_iota(jnp.int32, (length_in, length_out), 1)
    angles = (left_index * right_index % period).astype(jnp.float32) * (2.0 * jnp.pi / period)
    return (jnp.cos(angles), jnp.sin(angles))


def transform_first(cube, table):
    return jnp.einsum("cpq,pk->ckq", cube, table, precision=lax.Precision.HIGHEST)


def transform_second(cube, table):
    return jnp.einsum("ckq,qj->cjk", cube, table, precision=lax.Precision.HIGHEST)


def positional(real_part, imag_part):
    rows_count, seq_total = real_part.shape
    second_len = seq_total // FIRST_LEN
    cos_first, sin_first = dft_tables(FIRST_LEN, FIRST_LEN, FIRST_LEN)
    cos_twist, sin_twist = dft_tables(FIRST_LEN, second_len, seq_total)
    cos_second, sin_second = dft_tables(second_len, second_len, second_len)
    real_cube = real_part.reshape(rows_count, FIRST_LEN, second_len)
    imag_cube = imag_part.reshape(rows_count, FIRST_LEN, second_len)
    section_real = transform_first(real_cube, cos_first) + transform_first(imag_cube, sin_first)
    section_imag = transform_first(imag_cube, cos_first) - transform_first(real_cube, sin_first)
    twist_real = section_real * cos_twist + section_imag * sin_twist
    twist_imag = section_imag * cos_twist - section_real * sin_twist
    summed = transform_second(twist_real, cos_second) + transform_second(twist_imag, sin_second)
    norm_scale = 1.0 / jnp.sqrt(jnp.float32(seq_total * GROUP_WIDTH))
    return (summed.reshape(rows_count, seq_total) * norm_scale).astype(jnp.bfloat16)


def on_device(tokens, norm_gain, w_fourier_in, w_gate, w_spectrum, w_output):
    batches, seq_local, features = tokens.shape
    tokens_count = batches * seq_local
    widened = tokens.astype(jnp.float32)
    inverse = lax.rsqrt(jnp.mean(widened * widened, axis=-1, keepdims=True) + norm_eps)
    normed = (widened * inverse * norm_gain).astype(jnp.bfloat16).reshape(tokens_count, features)
    fourier_in = jnp.dot(normed, w_fourier_in, preferred_element_type=jnp.float32).astype(
        jnp.bfloat16
    )
    local_groups = w_fourier_in.shape[1] // GROUP_WIDTH
    grouped = fourier_in.astype(jnp.float32).reshape(batches, seq_local, local_groups, GROUP_WIDTH)
    cos_group, sin_group = dft_tables(GROUP_WIDTH, GROUP_WIDTH, GROUP_WIDTH)
    real_part = jnp.einsum(
        "btgn,nm->bgmt", grouped, cos_group, precision=lax.Precision.HIGHEST
    ).reshape(-1, seq_local)
    imag_part = -jnp.einsum(
        "btgn,nm->bgmt", grouped, sin_group, precision=lax.Precision.HIGHEST
    ).reshape(-1, seq_local)
    real_part = lax.all_to_all(
        shortened(real_part), "row", split_axis=0, concat_axis=1, tiled=True
    ).astype(real_part.dtype)
    imag_part = lax.all_to_all(
        shortened(imag_part), "row", split_axis=0, concat_axis=1, tiled=True
    ).astype(imag_part.dtype)
    spectrum = positional(real_part, imag_part)
    spectrum = lax.all_to_all(spectrum, "row", split_axis=1, concat_axis=0, tiled=True)
    spectrum = spectrum.reshape(batches, local_groups * GROUP_WIDTH, seq_local)
    spectrum = jnp.transpose(spectrum, (0, 2, 1)).reshape(tokens_count, local_groups * GROUP_WIDTH)

    def add_spectrum(running, portion, beginning):
        weight_rows = lax.dynamic_slice_in_dim(w_spectrum, beginning, portion.shape[1], 0)
        return running + jnp.dot(portion, weight_rows, preferred_element_type=jnp.float32)

    mixed_pre = over_all(
        spectrum, "col", 1, add_spectrum, jnp.zeros((tokens_count, features), jnp.float32)
    ).astype(jnp.bfloat16)
    gate_pre = jnp.dot(normed, w_gate, preferred_element_type=jnp.float32)
    mixed = (jax.nn.sigmoid(gate_pre) * mixed_pre.astype(jnp.float32)).astype(jnp.bfloat16)
    result = jnp.dot(mixed, w_output, preferred_element_type=jnp.float32)
    return result.astype(jnp.bfloat16).reshape(batches, seq_local, -1)


MESH = pl.DeviceIdType.MESH
HALF = GROUP_WIDTH // 2


def fold_table():
    n = np.arange(GROUP_WIDTH)
    table = np.zeros((2, HALF, GROUP_WIDTH))
    for m in range(HALF):
        table[0, m] = np.cos(2 * np.pi * (n * m % GROUP_WIDTH) / GROUP_WIDTH)
        table[1, m] = np.sin(2 * np.pi * (n * m % GROUP_WIDTH) / GROUP_WIDTH)
    table[1, 0] = np.cos(np.pi * n)
    return table.reshape(GROUP_WIDTH, GROUP_WIDTH)


def first_table(n1):
    a = np.arange(n1)
    ang = 2 * np.pi * (np.outer(a, a) % n1) / n1
    return np.concatenate([np.cos(ang), np.sin(ang)], 0)


def twist_table(n1, n2):
    phi = 2 * np.pi * np.outer(np.arange(n1), np.arange(n2)) / (n1 * n2)
    scale = 1.0 / np.sqrt(n1 * n2 * GROUP_WIDTH)
    return np.stack([np.cos(phi) * scale, np.sin(phi) * scale])


def second_table(rows, n2):
    q = np.arange(n2)
    psi = 2 * np.pi * (np.outer(q, q) % n2) / n2
    cos, sin = np.cos(psi), np.sin(psi)
    even = np.concatenate([cos, sin], 1)
    odd = np.concatenate([sin, -cos], 1)
    zero = np.zeros_like(even)
    plain = np.stack([np.concatenate([even, -odd], 1), np.concatenate([even, odd], 1)])
    first = np.stack([np.concatenate([even, zero], 1), np.concatenate([zero, even], 1)])
    both = np.stack([plain, first])
    per = n2 // rows
    both = both.reshape(2, 2, rows, per, 4 * n2).transpose(0, 3, 2, 1, 4)
    return both.reshape(2, 2 * n2, 4 * n2)


def channel_order(rows, cols):
    take = np.zeros((rows, cols, 2), np.int64)
    for r in range(rows):
        for c in range(cols):
            take[r, c, 0] = c * GROUP_WIDTH + r
            take[r, c, 1] = c * GROUP_WIDTH + (HALF if r == 0 else GROUP_WIDTH - r)
    return np.eye(rows * cols * 2)[take.reshape(-1)]


def row_offsets():
    far = lambda n: sorted(range(n), key=lambda d: -min(d, n - d))
    return [(dz, dy) for dz in far(8) for dy in far(4) if dz or dy]


def mixer_kernel(
    rows, cols, tok, gain_in, wf_in, wg_in, wspec_in, wout, fold_in, f1_in, f2_in, tw_in, perm_in, out,
    tokv, gain, wf, wg, wsv, ws, wo, fold, f1, f2, tw, perm, wp, gate, ysc, s1, x1, xs, zs, spec, osc,
    tsem, lsem, s1s, s1r, xss, xsr, s2s, s2r, oss, osr, wos, wor,
):
    batches, seq_local, features = tok.shape
    n1, n2 = tw.shape[1:]
    blocks = seq_local // n2
    span = seq_local // cols
    width = wout.shape[1]
    chunk = 512
    chunks = seq_local // chunk
    me = lax.axis_index("row")
    col = lax.axis_index("col")
    z, y = lax.div(me, 4), lax.rem(me, 4)
    sib = col + 1 - 2 * lax.rem(col, 2)
    peers = [lax.rem(z + dz, 8) * 4 + lax.rem(y + dy, 4) for dz, dy in row_offsets()]
    far = [lax.rem(col + 4, cols), lax.rem(sib + 4, cols)]
    near = [lax.rem(col + 2, cols), lax.rem(col + 6, cols), lax.rem(sib + 2, cols), lax.rem(sib + 6, cols)]
    others = far + near + [sib]

    def load(src, dst, at):
        copy = pltpu.make_async_copy(src, dst, lsem.at[at])
        copy.start()
        return copy

    def lane_block(c, size):
        return pl.ds(pl.multiple_of(c * size, size), size)

    fold_load = load(fold_in, fold, 0)
    wf_load = load(wf_in, wf, 1)
    gain_load = load(gain_in, gain, 2)
    loads = {}
    for b in range(batches):
        for j in range(chunks):
            part = pl.ds(j * chunk, chunk)
            loads[b, j] = pltpu.make_async_copy(tok.at[b, part], tokv.at[b, part], tsem.at[b, j])
            loads[b, j].start()
    wo_load = load(wout, wo.at[:, lane_block(col, width)], 3)
    wg_load = load(wg_in, wg, 4)
    spec_load = load(wspec_in, wsv, 5)
    perm_load = load(perm_in, perm, 6)
    f1_load = load(f1_in, f1, 7)
    tw_load = load(tw_in, tw, 8)
    f2_load = load(f2_in, f2, 9)

    barrier = pltpu.get_barrier_semaphore()
    for to in peers:
        pl.semaphore_signal(barrier, inc=1, device_id={"row": to}, device_id_type=MESH)
    for to in others:
        pl.semaphore_signal(barrier, inc=1, device_id={"col": to}, device_id_type=MESH)

    fold_load.wait()
    wf_load.wait()
    gain_load.wait()
    folded = jnp.zeros((GROUP_WIDTH, features), jnp.float32)
    for half in range(2):
        folded += lax.dot_general(
            fold[half], wf[...], (((1,), (1,)), ((), ())), preferred_element_type=jnp.float32
        )
    wp[...] = (folded * gain[...]).astype(jnp.bfloat16)

    def project(b):
        for j in range(chunks):
            loads[b, j].wait()
            t = tokv[b, j * chunk:(j + 1) * chunk, :]
            part = lax.dot_general(
                wp[...], t, (((1,), (1,)), ((), ())), preferred_element_type=jnp.float32
            )
            squares = jnp.zeros((chunk, LANES), jnp.float32)
            for k in range(features // LANES):
                w = t[:, k * LANES:(k + 1) * LANES].astype(jnp.float32)
                squares += w * w
            total = jnp.sum(squares.T, axis=0, keepdims=True)
            part = part * lax.rsqrt(total * (1.0 / features) + norm_eps)
            for k in range(chunk // n2):
                ysc[pl.ds(j * (chunk // n2) + k, GROUP_WIDTH, stride=blocks), :] = part[:, k * n2:(k + 1) * n2]
        for c in range(2):
            half = ysc[c * rows * blocks:(c + 1) * rows * blocks, :].reshape(rows, blocks, n2)
            s1[b, :, :, c * n2:(c + 1) * n2] = half.astype(jnp.bfloat16)

    def remote(src, dst, send, recv, to):
        return pltpu.make_async_remote_copy(
            src_ref=src, dst_ref=dst, send_sem=send, recv_sem=recv, device_id=to, device_id_type=MESH
        )

    def drain(ref, sem):
        pltpu.make_async_copy(ref, ref, sem).wait()

    def send_first(b):
        for to in peers:
            remote(s1.at[b, to], x1.at[b, me], s1s.at[b], s1r.at[b], {"row": to}).start()
        x1[b, me] = s1[b, me]

    def gates(b):
        t = tokv[b, pl.ds(pl.multiple_of(col * span, span), span), :].astype(jnp.float32)
        scale = lax.rsqrt(jnp.mean(t * t, axis=-1, keepdims=True) + norm_eps)
        normed = (t * scale * gain[...]).astype(jnp.bfloat16)
        g = jnp.dot(normed, wg[...], preferred_element_type=jnp.float32)
        gate[b] = 0.5 * jnp.tanh(0.5 * g) + 0.5

    def transform(b):
        x = x1[b].reshape(n1, 2 * n2)
        g = jnp.dot(f1[...], x, preferred_element_type=jnp.float32)
        cos, sin = tw[0], tw[1]
        parts = []
        for c in range(2):
            gc = g[:n1, c * n2:(c + 1) * n2]
            gs = g[n1:, c * n2:(c + 1) * n2]
            parts.append((gc * cos - gs * sin).astype(jnp.bfloat16))
            parts.append((-(gc * sin + gs * cos)).astype(jnp.bfloat16))
        t = jnp.concatenate(parts, axis=1)
        own = jnp.where(me == 0, 1, 0)
        o = lax.dot_general(
            f2[own], t, (((1,), (1,)), ((), ())), preferred_element_type=jnp.float32
        ).astype(jnp.bfloat16)
        for c in range(cols):
            k, h = divmod(c * span, n1)
            xs[b, c] = o[k * 2 * rows:(k + 1) * 2 * rows, h:h + span].reshape(rows, 2, span)

    def send_cross(b):
        for to in others:
            remote(xs.at[b, to], zs.at[b, :, col], xss.at[b], xsr.at[b], {"col": to}).start()
        zs[b, :, col] = xs[b, col]

    def send_second(b):
        drain(xs.at[b, pl.ds(0, cols - 1)], xsr.at[b])
        for to in peers:
            remote(zs.at[b, to], spec.at[b, me], s2s.at[b], s2r.at[b], {"row": to}).start()
        spec[b, me] = zs[b, me]

    def share(owner, at, to):
        part = wo.at[:, lane_block(owner, width)]
        return remote(part, part, wos.at[at], wor.at[at], {"col": to})

    def mix(b):
        drain(s1.at[b, pl.ds(0, rows - 1)], s2r.at[b])
        lhs = spec[b].reshape(2 * rows * cols, span)
        pre = lax.dot_general(
            lhs, ws[...], (((0,), (0,)), ((), ())), preferred_element_type=jnp.float32
        )
        return (gate[b] * pre).astype(jnp.bfloat16)

    def emit(b, mixed):
        for step in range(cols // 2):
            chip = lax.rem(lax.div(col, 2) + (2, 1, 3, 0)[step], cols // 2)
            res = jnp.dot(
                mixed, wo[:, lane_block(chip, 2 * width)], preferred_element_type=jnp.float32
            ).astype(jnp.bfloat16)
            for core in range(2):
                osc[b, chip * 2 + core] = res[:, core * width:(core + 1) * width]
            rest = pl.ds(pl.multiple_of(col * span, span), span)
            targets = (far, near[0::2], near[1::2], [sib])[step]
            for to in targets:
                remote(
                    osc.at[b, to], out.at[b, rest, :], oss.at[b], osr.at[b], {"col": to}
                ).start()
            if step == cols // 2 - 1:
                out[b, rest, :] = osc[b, col]

    project(0)
    pl.semaphore_wait(barrier, rows - 1 + cols - 1)
    send_first(0)
    wo_load.wait()
    share(col, 0, near[0]).start()
    share(col, 1, near[1]).start()
    share(col, 3, sib).start()
    for b in range(1, batches):
        project(b)
        send_first(b)
    wg_load.wait()
    for b in range(batches):
        gates(b)
    spec_load.wait()
    perm_load.wait()
    ws[...] = jnp.dot(perm[...], wsv[...], preferred_element_type=jnp.float32).astype(jnp.bfloat16)
    f1_load.wait()
    tw_load.wait()
    f2_load.wait()
    for b in range(batches):
        drain(s1.at[b, pl.ds(0, rows - 1)], s1r.at[b])
        transform(b)
        send_cross(b)
        if b == 0:
            share(col, 2, far[0]).start()
            share(near[1], 0, sib).wait_recv()
            share(near[1], 4, sib).start()
            share(near[0], 1, sib).wait_recv()
            share(near[0], 5, sib).start()
    for b in range(batches):
        send_second(b)
    share(far[0], 2, sib).wait_recv()
    share(far[0], 6, sib).start()
    for at in range(3, 7):
        share(col, at, sib).wait_recv()
    for b in range(batches):
        emit(b, mix(b))
    for b in range(batches):
        drain(osc.at[b, pl.ds(0, cols - 1)], osr.at[b])
    for b in range(batches):
        drain(s1.at[b, pl.ds(0, rows - 1)], s1s.at[b])
        drain(xs.at[b, pl.ds(0, cols - 1)], xss.at[b])
        drain(s1.at[b, pl.ds(0, rows - 1)], s2s.at[b])
        drain(osc.at[b, pl.ds(0, cols - 1)], oss.at[b])
    for at in range(7):
        share(col, at, sib).wait_send()


def fused(rows, cols, tokens, norm_gain, w_fourier_in, w_gate, w_spectrum, w_output):
    batches, seq_local, features = tokens.shape
    n2 = LANES
    n1 = seq_local * rows // n2
    blocks = seq_local // n2
    span = seq_local // cols
    width = w_output.shape[1]
    fold = fold_table()
    fold_high = fold.astype(jnp.bfloat16)
    fold_low = (fold - fold_high.astype(np.float64)).astype(jnp.bfloat16)
    tables = (
        jnp.asarray(np.stack([fold_high, fold_low])),
        jnp.asarray(first_table(n1), jnp.bfloat16),
        jnp.asarray(second_table(rows, n2), jnp.bfloat16),
        jnp.asarray(twist_table(n1, n2), jnp.float32),
        jnp.asarray(channel_order(rows, cols), jnp.bfloat16),
    )
    hbm = pl.BlockSpec(memory_space=pl.ANY)
    dma = pltpu.SemaphoreType.DMA
    half = jnp.bfloat16
    scratch = [
        (tokens.shape, half), ((1, features), jnp.float32), (w_fourier_in.shape, half),
        (w_gate.shape, half), (w_spectrum.shape, half), (w_spectrum.shape, half),
        ((features, features), half), *((t.shape, t.dtype) for t in tables),
        ((GROUP_WIDTH, features), half), ((batches, span, features), jnp.float32),
        ((GROUP_WIDTH * blocks, n2), jnp.float32),
        ((batches, rows, blocks, 2 * n2), half), ((batches, rows, blocks, 2 * n2), half),
        ((batches, cols, rows, 2, span), half), ((batches, rows, cols, 2, span), half),
        ((batches, rows, cols, 2, span), half), ((batches, cols, span, width), half),
    ]
    return pl.pallas_call(
        functools.partial(mixer_kernel, rows, cols),
        out_shape=jax.ShapeDtypeStruct((batches, seq_local, width), jnp.bfloat16),
        in_specs=[hbm] * 11,
        out_specs=pl.BlockSpec(memory_space=pltpu.VMEM),
        scratch_shapes=[pltpu.VMEM(shape, dtype) for shape, dtype in scratch] + [
            dma((batches, seq_local // 512)), dma((10,)),
            *(dma((batches,)) for _ in range(8)), dma((7,)), dma((7,)),
        ],
        compiler_params=pltpu.CompilerParams(
            collective_id=0, has_side_effects=True, vmem_limit_bytes=60 * 1024 * 1024
        ),
    )(tokens, norm_gain[None, :], w_fourier_in, w_gate, w_spectrum, w_output, *tables)


def body(rows, cols, *args):
    tokens, w_fourier_in, w_output = args[0], args[2], args[5]
    fits = (
        rows == HALF and cols == 8 and w_fourier_in.shape[1] == GROUP_WIDTH
        and tokens.shape[1:] == (16 * LANES, 8 * LANES) and w_output.shape[1] == LANES
    )
    if fits:
        return fused(rows, cols, *args)
    return on_device(*args)


def solution(mesh):
    placed = (P(None, "row", None), P(), P(None, "col"), P(), P(), P(None, "col"))
    return jax.shard_map(
        functools.partial(body, mesh.shape["row"], mesh.shape["col"]),
        mesh=mesh, in_specs=placed, out_specs=P(None, "row", "col"), check_vma=False,
    )
```

```python
import functools

import jax
import jax.numpy as jnp
import numpy as np
from jax import lax
from jax.experimental import pallas as pl
from jax.experimental.pallas import tpu as pltpu
from jax.sharding import PartitionSpec as P

GROUP_WIDTH = 64
FIRST_LEN = 256
LANES = 128


norm_eps = 1e-06


def shortened(value):
    return jax.tree.map(lambda a: a.astype(jnp.bfloat16) if a.dtype == jnp.float32 else a, value)


def over_all(value, axis, dim, absorb, carry):
    whole = jax.tree.map(lambda part: lax.all_gather(part, axis, axis=dim, tiled=True), value)
    return absorb(carry, whole, jnp.int32(0))


def dft_tables(length_in, length_out, period):
    left_index = lax.broadcasted_iota(jnp.int32, (length_in, length_out), 0)
    right_index = lax.broadcasted_iota(jnp.int32, (length_in, length_out), 1)
    angles = (left_index * right_index % period).astype(jnp.float32) * (2.0 * jnp.pi / period)
    return (jnp.cos(angles), jnp.sin(angles))


def transform_first(cube, table):
    return jnp.einsum("cpq,pk->ckq", cube, table, precision=lax.Precision.HIGHEST)


def transform_second(cube, table):
    return jnp.einsum("ckq,qj->cjk", cube, table, precision=lax.Precision.HIGHEST)


def positional(real_part, imag_part):
    rows_count, seq_total = real_part.shape
    second_len = seq_total // FIRST_LEN
    cos_first, sin_first = dft_tables(FIRST_LEN, FIRST_LEN, FIRST_LEN)
    cos_twist, sin_twist = dft_tables(FIRST_LEN, second_len, seq_total)
    cos_second, sin_second = dft_tables(second_len, second_len, second_len)
    real_cube = real_part.reshape(rows_count, FIRST_LEN, second_len)
    imag_cube = imag_part.reshape(rows_count, FIRST_LEN, second_len)
    section_real = transform_first(real_cube, cos_first) + transform_first(imag_cube, sin_first)
    section_imag = transform_first(imag_cube, cos_first) - transform_first(real_cube, sin_first)
    twist_real = section_real * cos_twist + section_imag * sin_twist
    twist_imag = section_imag * cos_twist - section_real * sin_twist
    summed = transform_second(twist_real, cos_second) + transform_second(twist_imag, sin_second)
    norm_scale = 1.0 / jnp.sqrt(jnp.float32(seq_total * GROUP_WIDTH))
    return (summed.reshape(rows_count, seq_total) * norm_scale).astype(jnp.bfloat16)


def on_device(tokens, norm_gain, w_fourier_in, w_gate, w_spectrum, w_output):
    batches, seq_local, features = tokens.shape
    tokens_count = batches * seq_local
    widened = tokens.astype(jnp.float32)
    inverse = lax.rsqrt(jnp.mean(widened * widened, axis=-1, keepdims=True) + norm_eps)
    normed = (widened * inverse * norm_gain).astype(jnp.bfloat16).reshape(tokens_count, features)
    fourier_in = jnp.dot(normed, w_fourier_in, preferred_element_type=jnp.float32).astype(
        jnp.bfloat16
    )
    local_groups = w_fourier_in.shape[1] // GROUP_WIDTH
    grouped = fourier_in.astype(jnp.float32).reshape(batches, seq_local, local_groups, GROUP_WIDTH)
    cos_group, sin_group = dft_tables(GROUP_WIDTH, GROUP_WIDTH, GROUP_WIDTH)
    real_part = jnp.einsum(
        "btgn,nm->bgmt", grouped, cos_group, precision=lax.Precision.HIGHEST
    ).reshape(-1, seq_local)
    imag_part = -jnp.einsum(
        "btgn,nm->bgmt", grouped, sin_group, precision=lax.Precision.HIGHEST
    ).reshape(-1, seq_local)
    real_part = lax.all_to_all(
        shortened(real_part), "row", split_axis=0, concat_axis=1, tiled=True
    ).astype(real_part.dtype)
    imag_part = lax.all_to_all(
        shortened(imag_part), "row", split_axis=0, concat_axis=1, tiled=True
    ).astype(imag_part.dtype)
    spectrum = positional(real_part, imag_part)
    spectrum = lax.all_to_all(spectrum, "row", split_axis=1, concat_axis=0, tiled=True)
    spectrum = spectrum.reshape(batches, local_groups * GROUP_WIDTH, seq_local)
    spectrum = jnp.transpose(spectrum, (0, 2, 1)).reshape(tokens_count, local_groups * GROUP_WIDTH)

    def add_spectrum(running, portion, beginning):
        weight_rows = lax.dynamic_slice_in_dim(w_spectrum, beginning, portion.shape[1], 0)
        return running + jnp.dot(portion, weight_rows, preferred_element_type=jnp.float32)

    mixed_pre = over_all(
        spectrum, "col", 1, add_spectrum, jnp.zeros((tokens_count, features), jnp.float32)
    ).astype(jnp.bfloat16)
    gate_pre = jnp.dot(normed, w_gate, preferred_element_type=jnp.float32)
    mixed = (jax.nn.sigmoid(gate_pre) * mixed_pre.astype(jnp.float32)).astype(jnp.bfloat16)
    result = jnp.dot(mixed, w_output, preferred_element_type=jnp.float32)
    return result.astype(jnp.bfloat16).reshape(batches, seq_local, -1)


MESH = pl.DeviceIdType.MESH
HALF = GROUP_WIDTH // 2


def fold_table():
    n = np.arange(GROUP_WIDTH)
    table = np.zeros((2, HALF, GROUP_WIDTH))
    for m in range(HALF):
        table[0, m] = np.cos(2 * np.pi * (n * m % GROUP_WIDTH) / GROUP_WIDTH)
        table[1, m] = np.sin(2 * np.pi * (n * m % GROUP_WIDTH) / GROUP_WIDTH)
    table[1, 0] = np.cos(np.pi * n)
    return table.reshape(GROUP_WIDTH, GROUP_WIDTH)


def first_table(n1):
    a = np.arange(n1)
    ang = 2 * np.pi * (np.outer(a, a) % n1) / n1
    return np.concatenate([np.cos(ang), np.sin(ang)], 0)


def twist_table(n1, n2):
    phi = 2 * np.pi * np.outer(np.arange(n1), np.arange(n2)) / (n1 * n2)
    scale = 1.0 / np.sqrt(n1 * n2 * GROUP_WIDTH)
    return np.stack([np.cos(phi) * scale, np.sin(phi) * scale])


def second_table(rows, n2):
    q = np.arange(n2)
    psi = 2 * np.pi * (np.outer(q, q) % n2) / n2
    cos, sin = np.cos(psi), np.sin(psi)
    even = np.concatenate([cos, sin], 1)
    odd = np.concatenate([sin, -cos], 1)
    zero = np.zeros_like(even)
    plain = np.stack([np.concatenate([even, -odd], 1), np.concatenate([even, odd], 1)])
    first = np.stack([np.concatenate([even, zero], 1), np.concatenate([zero, even], 1)])
    both = np.stack([plain, first])
    per = n2 // rows
    both = both.reshape(2, 2, rows, per, 4 * n2).transpose(0, 3, 2, 1, 4)
    return both.reshape(2, 2 * n2, 4 * n2)


def channel_order(rows, cols):
    take = np.zeros((rows, cols, 2), np.int64)
    for r in range(rows):
        for c in range(cols):
            take[r, c, 0] = c * GROUP_WIDTH + r
            take[r, c, 1] = c * GROUP_WIDTH + (HALF if r == 0 else GROUP_WIDTH - r)
    return np.eye(rows * cols * 2)[take.reshape(-1)]


def row_offsets():
    far = lambda n: sorted(range(n), key=lambda d: -min(d, n - d))
    return [(dz, dy) for dz in far(8) for dy in far(4) if dz or dy]


def mixer_kernel(
    rows, cols, tok, gain_in, wf_in, wg_in, wspec_in, wout, fold_in, f1_in, f2_in, tw_in, perm_in, out,
    tokv, gain, wf, wg, wsv, ws, wo, fold, f1, f2, tw, perm, wp, gate, ysc, s1, x1, xs, ps, spec, osc,
    tsem, lsem, s1s, s1r, sws, swr, s2s, s2r, oss, osr, wos, wor,
):
    batches, seq_local, features = tok.shape
    n1, n2 = tw.shape[1:]
    blocks = seq_local // n2
    span = seq_local // cols
    width = wout.shape[1]
    chunk = 512
    chunks = seq_local // chunk
    me = lax.axis_index("row")
    col = lax.axis_index("col")
    z, y = lax.div(me, 4), lax.rem(me, 4)
    sib = col + 1 - 2 * lax.rem(col, 2)
    peers = [lax.rem(z + dz, 8) * 4 + lax.rem(y + dy, 4) for dz, dy in row_offsets()]
    far = [lax.rem(col + 4, cols), lax.rem(sib + 4, cols)]
    near = [lax.rem(col + 2, cols), lax.rem(col + 6, cols), lax.rem(sib + 2, cols), lax.rem(sib + 6, cols)]
    others = far + near + [sib]
    same = [far[0], near[0], near[1]]
    core = lax.rem(col, 2)

    def load(src, dst, at):
        copy = pltpu.make_async_copy(src, dst, lsem.at[at])
        copy.start()
        return copy

    def lane_block(c, size):
        return pl.ds(pl.multiple_of(c * size, size), size)

    fold_load = load(fold_in, fold, 0)
    wf_load = load(wf_in, wf, 1)
    gain_load = load(gain_in, gain, 2)
    loads = {}
    for b in range(batches):
        for j in range(chunks):
            part = pl.ds(j * chunk, chunk)
            loads[b, j] = pltpu.make_async_copy(tok.at[b, part], tokv.at[b, part], tsem.at[b, j])
            loads[b, j].start()
    wo_load = load(wout, wo.at[:, lane_block(col, width)], 3)
    wg_load = load(wg_in, wg, 4)
    spec_load = load(wspec_in, wsv, 5)
    perm_load = load(perm_in, perm, 6)
    f1_load = load(f1_in, f1, 7)
    tw_load = load(tw_in, tw, 8)
    f2_load = load(f2_in, f2, 9)

    barrier = pltpu.get_barrier_semaphore()
    for to in peers:
        pl.semaphore_signal(barrier, inc=1, device_id={"row": to}, device_id_type=MESH)
    for to in others:
        pl.semaphore_signal(barrier, inc=1, device_id={"col": to}, device_id_type=MESH)

    fold_load.wait()
    wf_load.wait()
    gain_load.wait()
    folded = jnp.zeros((GROUP_WIDTH, features), jnp.float32)
    for half in range(2):
        folded += lax.dot_general(
            fold[half], wf[...], (((1,), (0,)), ((), ())), preferred_element_type=jnp.float32
        )
    wp[...] = (folded * gain[...]).astype(jnp.bfloat16)

    def project(b):
        for j in range(chunks):
            loads[b, j].wait()
            t = tokv[b, j * chunk:(j + 1) * chunk, :]
            part = lax.dot_general(
                wp[...], t, (((1,), (1,)), ((), ())), preferred_element_type=jnp.float32
            )
            squares = jnp.zeros((chunk, LANES), jnp.float32)
            for k in range(features // LANES):
                w = t[:, k * LANES:(k + 1) * LANES].astype(jnp.float32)
                squares += w * w
            total = jnp.sum(squares.T, axis=0, keepdims=True)
            part = part * lax.rsqrt(total * (1.0 / features) + norm_eps)
            for k in range(chunk // n2):
                ysc[pl.ds(j * (chunk // n2) + k, GROUP_WIDTH, stride=blocks), :] = part[:, k * n2:(k + 1) * n2]
        for c in range(2):
            half = ysc[c * rows * blocks:(c + 1) * rows * blocks, :].reshape(rows, blocks, n2)
            s1[b, :, :, c * n2:(c + 1) * n2] = half.astype(jnp.bfloat16)

    def remote(src, dst, send, recv, to):
        return pltpu.make_async_remote_copy(
            src_ref=src, dst_ref=dst, send_sem=send, recv_sem=recv, device_id=to, device_id_type=MESH
        )

    def drain(ref, sem):
        pltpu.make_async_copy(ref, ref, sem).wait()

    def send_first(b):
        for to in peers:
            remote(s1.at[b, to], x1.at[b, me], s1s.at[b], s1r.at[b], {"row": to}).start()
        x1[b, me] = s1[b, me]

    def gates(b):
        t = tokv[b, pl.ds(pl.multiple_of(col * span, span), span), :].astype(jnp.float32)
        scale = lax.rsqrt(jnp.mean(t * t, axis=-1, keepdims=True) + norm_eps)
        normed = (t * scale * gain[...]).astype(jnp.bfloat16)
        g = jnp.dot(normed, wg[...], preferred_element_type=jnp.float32)
        gate[b] = 0.5 * jnp.tanh(0.5 * g) + 0.5

    def transform(b):
        x = x1[b].reshape(n1, 2 * n2)
        g = jnp.dot(f1[...], x, preferred_element_type=jnp.float32)
        cos, sin = tw[0], tw[1]
        parts = []
        for c in range(2):
            gc = g[:n1, c * n2:(c + 1) * n2]
            gs = g[n1:, c * n2:(c + 1) * n2]
            parts.append((gc * cos - gs * sin).astype(jnp.bfloat16))
            parts.append((-(gc * sin + gs * cos)).astype(jnp.bfloat16))
        t = jnp.concatenate(parts, axis=1)
        own = jnp.where(me == 0, 1, 0)
        o = lax.dot_general(
            f2[own], t, (((1,), (1,)), ((), ())), preferred_element_type=jnp.float32
        )
        low, high = o[:, :span], o[:, span:]
        mine = jnp.where(core == 0, low, high)
        other = jnp.where(core == 0, high, low)
        ps[b, :, core] = mine.astype(jnp.bfloat16).reshape(rows * cols // 2, 2, span)
        xs[b] = other.astype(jnp.bfloat16).reshape(rows * cols // 2, 2, span)

    def swap(b):
        return remote(
            xs.at[b], ps.at[b, :, core], sws.at[b], swr.at[b], {"col": sib}
        )

    def send_second(b):
        def one(to, c):
            remote(
                ps.at[b, lax.div(c, 2) * rows + to], spec.at[b, me, lax.div(col, 2)],
                s2s.at[b], s2r.at[b], {"row": to, "col": c},
            ).start()

        def per_row(i, carry):
            step = lax.div(i, 4)
            dz = 4 + lax.div(step + 1, 2) * (1 - 2 * lax.rem(step, 2))
            dy = 2 + lax.div(lax.rem(i, 4) + 1, 2) * (1 - 2 * lax.rem(i, 2))
            to = lax.rem(z + dz, 8) * 4 + lax.rem(y + dy, 4)
            for c in same:
                one(to, c)
            one(to, col)
            return carry

        lax.fori_loop(0, rows - 1, per_row, 0)
        for c in same:
            one(me, c)
        spec[b, me, lax.div(col, 2)] = ps[b, lax.div(col, 2) * rows + me]

    def share(owner, at, to):
        part = wo.at[:, lane_block(owner, width)]
        return remote(part, part, wos.at[at], wor.at[at], {"col": to})

    def mix(b):
        lhs = spec[b].reshape(2 * rows * cols, span)
        pre = lax.dot_general(
            lhs, ws[...], (((0,), (0,)), ((), ())), preferred_element_type=jnp.float32
        )
        return (gate[b] * pre).astype(jnp.bfloat16)

    def emit(b, mixed):
        for step in range(cols // 2):
            chip = lax.rem(lax.div(col, 2) + (2, 1, 3, 0)[step], cols // 2)
            res = jnp.dot(
                mixed, wo[:, lane_block(chip, 2 * width)], preferred_element_type=jnp.float32
            ).astype(jnp.bfloat16)
            for core in range(2):
                osc[b, chip * 2 + core] = res[:, core * width:(core + 1) * width]
            rest = pl.ds(pl.multiple_of(col * span, span), span)
            targets = (far, near[0::2], near[1::2], [sib])[step]
            for to in targets:
                remote(
                    osc.at[b, to], out.at[b, rest, :], oss.at[b], osr.at[b], {"col": to}
                ).start()
            if step == cols // 2 - 1:
                out[b, rest, :] = osc[b, col]

    scope = jax.named_scope
    with scope("project0"):
        project(0)
    with scope("barrier"):
        pl.semaphore_wait(barrier, rows - 1 + cols - 1)
    with scope("send0"):
        send_first(0)
    wo_load.wait()
    share(col, 0, near[0]).start()
    share(col, 1, near[1]).start()
    share(col, 2, far[0]).start()
    share(col, 3, sib).start()
    with scope("gates"):
        wg_load.wait()
        gates(0)
    with scope("spectrum_rows"):
        spec_load.wait()
        perm_load.wait()
        ws[...] = jnp.dot(
            perm[...], wsv[...], preferred_element_type=jnp.float32
        ).astype(jnp.bfloat16)
        f1_load.wait()
        tw_load.wait()
        f2_load.wait()
    for b in range(1, batches):
        with scope("project%d" % b):
            project(b)
        with scope("send%d" % b):
            send_first(b)
        with scope("gates"):
            gates(b)
    for b in range(batches):
        with scope("wait_first%d" % b):
            drain(s1.at[b, pl.ds(0, rows - 1)], s1r.at[b])
        with scope("transform%d" % b):
            transform(b)
        with scope("swap%d" % b):
            swap(b).start()
            swap(b).wait_recv()
        with scope("second%d" % b):
            send_second(b)
        if b == 0:
            with scope("share"):
                share(near[1], 0, sib).wait_recv()
                share(near[1], 4, sib).start()
                share(near[0], 1, sib).wait_recv()
                share(near[0], 5, sib).start()
    with scope("share2"):
        share(far[0], 2, sib).wait_recv()
        share(far[0], 6, sib).start()
        for at in range(3, 7):
            share(col, at, sib).wait_recv()
    for b in range(batches):
        with scope("wait_second%d" % b):
            drain(ps.at[b, pl.ds(0, rows * cols // 2 - 1)], s2r.at[b])
        with scope("mix%d" % b):
            mixed = mix(b)
        with scope("emit%d" % b):
            emit(b, mixed)
    with scope("wait_out"):
        for b in range(batches):
            drain(osc.at[b, pl.ds(0, cols - 1)], osr.at[b])
    with scope("tail"):
        for b in range(batches):
            drain(s1.at[b, pl.ds(0, rows - 1)], s1s.at[b])
            drain(ps.at[b, pl.ds(0, rows * cols // 2 - 1)], s2s.at[b])
            swap(b).wait_send()
            drain(osc.at[b, pl.ds(0, cols - 1)], oss.at[b])
        for at in range(7):
            share(col, at, sib).wait_send()


def fused(rows, cols, tokens, norm_gain, w_fourier_in, w_gate, w_spectrum, w_output):
    batches, seq_local, features = tokens.shape
    n2 = LANES
    n1 = seq_local * rows // n2
    blocks = seq_local // n2
    span = seq_local // cols
    width = w_output.shape[1]
    fold = fold_table()
    fold_high = fold.astype(jnp.bfloat16)
    fold_low = (fold - fold_high.astype(np.float64)).astype(jnp.bfloat16)
    tables = (
        jnp.asarray(np.stack([fold_high, fold_low])),
        jnp.asarray(first_table(n1), jnp.bfloat16),
        jnp.asarray(second_table(rows, n2), jnp.bfloat16),
        jnp.asarray(twist_table(n1, n2), jnp.float32),
        jnp.asarray(channel_order(rows, cols), jnp.bfloat16),
    )
    hbm = pl.BlockSpec(memory_space=pltpu.HBM)
    dma = pltpu.SemaphoreType.DMA
    half = jnp.bfloat16
    scratch = [
        (tokens.shape, half), ((1, features), jnp.float32), (w_fourier_in.shape[::-1], half),
        (w_gate.shape, half), (w_spectrum.shape, half), (w_spectrum.shape, half),
        ((features, features), half), *((t.shape, t.dtype) for t in tables),
        ((GROUP_WIDTH, features), half), ((batches, span, features), jnp.float32),
        ((GROUP_WIDTH * blocks, n2), jnp.float32),
        ((batches, rows, blocks, 2 * n2), half), ((batches, rows, blocks, 2 * n2), half),
        ((batches, cols // 2 * rows, 2, span), half),
        ((batches, cols // 2 * rows, 2, 2, span), half),
        ((batches, rows, cols // 2, 2, 2, span), half),
        ((batches, cols, span, width), half),
    ]
    return pl.pallas_call(
        functools.partial(mixer_kernel, rows, cols),
        out_shape=pltpu.VMEM((batches, seq_local, width), jnp.bfloat16),
        in_specs=[hbm] * 11,
        out_specs=pl.BlockSpec(memory_space=pltpu.VMEM),
        scratch_shapes=[pltpu.VMEM(shape, dtype) for shape, dtype in scratch] + [
            dma((batches, seq_local // 512)), dma((10,)),
            *(dma((batches,)) for _ in range(8)), dma((7,)), dma((7,)),
        ],
        compiler_params=pltpu.CompilerParams(
            collective_id=0, has_side_effects=True, vmem_limit_bytes=62 * 1024 * 1024
        ),
    )(tokens, norm_gain[None, :], w_fourier_in.T, w_gate, w_spectrum, w_output, *tables)


def body(rows, cols, *args):
    tokens, w_fourier_in, w_output = args[0], args[2], args[5]
    fits = (
        rows == HALF and cols == 8 and w_fourier_in.shape[1] == GROUP_WIDTH
        and tokens.shape[1:] == (16 * LANES, 8 * LANES) and w_output.shape[1] == LANES
    )
    if fits:
        return fused(rows, cols, *args)
    return on_device(*args)


def solution(mesh):
    placed = (P(None, "row", None), P(), P(None, "col"), P(), P(), P(None, "col"))
    return jax.shard_map(
        functools.partial(body, mesh.shape["row"], mesh.shape["col"]),
        mesh=mesh, in_specs=placed, out_specs=P(None, "row", "col"), check_vma=False,
    )
```

```python
import functools

import jax
import jax.numpy as jnp
import numpy as np
from jax import lax
from jax.experimental import pallas as pl
from jax.experimental.pallas import tpu as pltpu
from jax.sharding import PartitionSpec as P

GROUP_WIDTH = 64
FIRST_LEN = 256
LANES = 128


norm_eps = 1e-06


def shortened(value):
    return jax.tree.map(lambda a: a.astype(jnp.bfloat16) if a.dtype == jnp.float32 else a, value)


def over_all(value, axis, dim, absorb, carry):
    whole = jax.tree.map(lambda part: lax.all_gather(part, axis, axis=dim, tiled=True), value)
    return absorb(carry, whole, jnp.int32(0))


def dft_tables(length_in, length_out, period):
    left_index = lax.broadcasted_iota(jnp.int32, (length_in, length_out), 0)
    right_index = lax.broadcasted_iota(jnp.int32, (length_in, length_out), 1)
    angles = (left_index * right_index % period).astype(jnp.float32) * (2.0 * jnp.pi / period)
    return (jnp.cos(angles), jnp.sin(angles))


def transform_first(cube, table):
    return jnp.einsum("cpq,pk->ckq", cube, table, precision=lax.Precision.HIGHEST)


def transform_second(cube, table):
    return jnp.einsum("ckq,qj->cjk", cube, table, precision=lax.Precision.HIGHEST)


def positional(real_part, imag_part):
    rows_count, seq_total = real_part.shape
    second_len = seq_total // FIRST_LEN
    cos_first, sin_first = dft_tables(FIRST_LEN, FIRST_LEN, FIRST_LEN)
    cos_twist, sin_twist = dft_tables(FIRST_LEN, second_len, seq_total)
    cos_second, sin_second = dft_tables(second_len, second_len, second_len)
    real_cube = real_part.reshape(rows_count, FIRST_LEN, second_len)
    imag_cube = imag_part.reshape(rows_count, FIRST_LEN, second_len)
    section_real = transform_first(real_cube, cos_first) + transform_first(imag_cube, sin_first)
    section_imag = transform_first(imag_cube, cos_first) - transform_first(real_cube, sin_first)
    twist_real = section_real * cos_twist + section_imag * sin_twist
    twist_imag = section_imag * cos_twist - section_real * sin_twist
    summed = transform_second(twist_real, cos_second) + transform_second(twist_imag, sin_second)
    norm_scale = 1.0 / jnp.sqrt(jnp.float32(seq_total * GROUP_WIDTH))
    return (summed.reshape(rows_count, seq_total) * norm_scale).astype(jnp.bfloat16)


def on_device(tokens, norm_gain, w_fourier_in, w_gate, w_spectrum, w_output):
    batches, seq_local, features = tokens.shape
    tokens_count = batches * seq_local
    widened = tokens.astype(jnp.float32)
    inverse = lax.rsqrt(jnp.mean(widened * widened, axis=-1, keepdims=True) + norm_eps)
    normed = (widened * inverse * norm_gain).astype(jnp.bfloat16).reshape(tokens_count, features)
    fourier_in = jnp.dot(normed, w_fourier_in, preferred_element_type=jnp.float32).astype(
        jnp.bfloat16
    )
    local_groups = w_fourier_in.shape[1] // GROUP_WIDTH
    grouped = fourier_in.astype(jnp.float32).reshape(batches, seq_local, local_groups, GROUP_WIDTH)
    cos_group, sin_group = dft_tables(GROUP_WIDTH, GROUP_WIDTH, GROUP_WIDTH)
    real_part = jnp.einsum(
        "btgn,nm->bgmt", grouped, cos_group, precision=lax.Precision.HIGHEST
    ).reshape(-1, seq_local)
    imag_part = -jnp.einsum(
        "btgn,nm->bgmt", grouped, sin_group, precision=lax.Precision.HIGHEST
    ).reshape(-1, seq_local)
    real_part = lax.all_to_all(
        shortened(real_part), "row", split_axis=0, concat_axis=1, tiled=True
    ).astype(real_part.dtype)
    imag_part = lax.all_to_all(
        shortened(imag_part), "row", split_axis=0, concat_axis=1, tiled=True
    ).astype(imag_part.dtype)
    spectrum = positional(real_part, imag_part)
    spectrum = lax.all_to_all(spectrum, "row", split_axis=1, concat_axis=0, tiled=True)
    spectrum = spectrum.reshape(batches, local_groups * GROUP_WIDTH, seq_local)
    spectrum = jnp.transpose(spectrum, (0, 2, 1)).reshape(tokens_count, local_groups * GROUP_WIDTH)

    def add_spectrum(running, portion, beginning):
        weight_rows = lax.dynamic_slice_in_dim(w_spectrum, beginning, portion.shape[1], 0)
        return running + jnp.dot(portion, weight_rows, preferred_element_type=jnp.float32)

    mixed_pre = over_all(
        spectrum, "col", 1, add_spectrum, jnp.zeros((tokens_count, features), jnp.float32)
    ).astype(jnp.bfloat16)
    gate_pre = jnp.dot(normed, w_gate, preferred_element_type=jnp.float32)
    mixed = (jax.nn.sigmoid(gate_pre) * mixed_pre.astype(jnp.float32)).astype(jnp.bfloat16)
    result = jnp.dot(mixed, w_output, preferred_element_type=jnp.float32)
    return result.astype(jnp.bfloat16).reshape(batches, seq_local, -1)


MESH = pl.DeviceIdType.MESH
HALF = GROUP_WIDTH // 2


def fold_table():
    n = np.arange(GROUP_WIDTH)
    table = np.zeros((2, HALF, GROUP_WIDTH))
    for m in range(HALF):
        table[0, m] = np.cos(2 * np.pi * (n * m % GROUP_WIDTH) / GROUP_WIDTH)
        table[1, m] = np.sin(2 * np.pi * (n * m % GROUP_WIDTH) / GROUP_WIDTH)
    table[1, 0] = np.cos(np.pi * n)
    return table.reshape(GROUP_WIDTH, GROUP_WIDTH)


def first_table(n1):
    a = np.arange(n1)
    ang = 2 * np.pi * (np.outer(a, a) % n1) / n1
    return np.concatenate([np.cos(ang), np.sin(ang)], 0)


def twist_table(n1, n2):
    phi = 2 * np.pi * np.outer(np.arange(n1), np.arange(n2)) / (n1 * n2)
    scale = 1.0 / np.sqrt(n1 * n2 * GROUP_WIDTH)
    return np.stack([np.cos(phi) * scale, np.sin(phi) * scale])


def second_table(rows, n2):
    q = np.arange(n2)
    psi = 2 * np.pi * (np.outer(q, q) % n2) / n2
    cos, sin = np.cos(psi), np.sin(psi)
    even = np.concatenate([cos, sin], 1)
    odd = np.concatenate([sin, -cos], 1)
    zero = np.zeros_like(even)
    plain = np.stack([np.concatenate([even, -odd], 1), np.concatenate([even, odd], 1)])
    first = np.stack([np.concatenate([even, zero], 1), np.concatenate([zero, even], 1)])
    both = np.stack([plain, first])
    per = n2 // rows
    both = both.reshape(2, 2, rows, per, 4 * n2).transpose(0, 3, 2, 1, 4)
    return both.reshape(2, 2 * n2, 4 * n2)


def channel_order(rows, cols):
    take = np.zeros((rows, cols, 2), np.int64)
    for r in range(rows):
        for c in range(cols):
            group = (c + 1 - 2 * (c % 2)) * GROUP_WIDTH
            take[r, c, 0] = group + r
            take[r, c, 1] = group + (HALF if r == 0 else GROUP_WIDTH - r)
    return np.eye(rows * cols * 2)[take.reshape(-1)]


def row_offsets():
    far = lambda n: sorted(range(n), key=lambda d: -min(d, n - d))
    return [(dz, dy) for dy in far(4) for dz in far(8) if dz or dy]


def mixer_kernel(
    rows, cols, tok, gain_in, wf_in, wg_in, wspec_in, wout, fold_in, f1_in, f2_in, tw_in, perm_in, out,
    tokv, gain, wf, wg, wsv, ws, wo, fold, f1, f2, tw, perm, wp, gate, ysc, tt, s1, x1, xs, ps, spec, osc,
    tsem, lsem, s1s, s1r, sws, swr, s2s, s2r, oss, osr, wos, wor,
):
    batches, seq_local, features = tok.shape
    n1, n2 = tw.shape[1:]
    blocks = seq_local // n2
    span = seq_local // cols
    width = wout.shape[1]
    chunk = 512
    chunks = seq_local // chunk
    me = lax.axis_index("row")
    col = lax.axis_index("col")
    z, y = lax.div(me, 4), lax.rem(me, 4)
    sib = col + 1 - 2 * lax.rem(col, 2)
    peers = [lax.rem(z + dz, 8) * 4 + lax.rem(y + dy, 4) for dz, dy in row_offsets()]
    far = [lax.rem(col + 4, cols), lax.rem(sib + 4, cols)]
    near = [lax.rem(col + 2, cols), lax.rem(col + 6, cols), lax.rem(sib + 2, cols), lax.rem(sib + 6, cols)]
    others = far + near + [sib]
    across = [far[1], near[2], near[3]]
    core = lax.rem(col, 2)

    turns = [z * 4 + lax.rem(y + d, 4) for d in range(1, 4)]

    def load(src, dst, at):
        copy = pltpu.make_async_copy(src, dst, lsem.at[at])
        copy.start()
        return copy

    def lane_block(c, size):
        return pl.ds(pl.multiple_of(c * size, size), size)

    barrier = pltpu.get_barrier_semaphore()
    for to in peers:
        pl.semaphore_signal(
            barrier, inc=1, device_id={"row": to, "col": sib}, device_id_type=MESH
        )
    for to in turns:
        pl.semaphore_signal(barrier, inc=1, device_id={"row": to}, device_id_type=MESH)
    for to in others:
        pl.semaphore_signal(barrier, inc=1, device_id={"col": to}, device_id_type=MESH)

    fold_load = load(fold_in, fold, 0)
    wf_load = load(wf_in, wf, 1)
    gain_load = load(gain_in, gain, 2)
    loads = {}
    for b in range(batches):
        for j in range(chunks):
            part = pl.ds(j * chunk, chunk)
            loads[b, j] = pltpu.make_async_copy(tok.at[b, part], tokv.at[b, part], tsem.at[b, j])
            loads[b, j].start()
    wo_load = load(wout, wo.at[:, lane_block(col, width)], 3)
    wg_load = load(wg_in, wg, 4)
    spec_load = load(wspec_in, wsv, 5)
    perm_load = load(perm_in, perm, 6)
    f1_load = load(f1_in, f1, 7)
    tw_load = load(tw_in, tw, 8)
    f2_load = load(f2_in, f2, 9)

    fold_load.wait()
    wf_load.wait()
    gain_load.wait()
    folded = jnp.zeros((GROUP_WIDTH, features), jnp.float32)
    for half in range(2):
        folded += lax.dot_general(
            fold[half], wf[...], (((1,), (0,)), ((), ())), preferred_element_type=jnp.float32
        )
    wp[...] = (folded * gain[...]).astype(jnp.bfloat16)

    def project(b):
        for j in range(chunks):
            loads[b, j].wait()
            t = tokv[b, j * chunk:(j + 1) * chunk, :]
            part = lax.dot_general(
                wp[...], t, (((1,), (1,)), ((), ())), preferred_element_type=jnp.float32
            )
            squares = jnp.zeros((chunk, LANES), jnp.float32)
            for k in range(features // LANES):
                w = t[:, k * LANES:(k + 1) * LANES].astype(jnp.float32)
                squares += w * w
            total = jnp.sum(squares.T, axis=0, keepdims=True)
            part = part * lax.rsqrt(total * (1.0 / features) + norm_eps)
            for k in range(chunk // n2):
                ysc[pl.ds(j * (chunk // n2) + k, GROUP_WIDTH, stride=blocks), :] = part[:, k * n2:(k + 1) * n2]
        for c in range(2):
            half = ysc[c * rows * blocks:(c + 1) * rows * blocks, :].reshape(rows, blocks, n2)
            s1[b, :, :, c * n2:(c + 1) * n2] = half.astype(jnp.bfloat16)

    def remote(src, dst, send, recv, to):
        return pltpu.make_async_remote_copy(
            src_ref=src, dst_ref=dst, send_sem=send, recv_sem=recv, device_id=to, device_id_type=MESH
        )

    def drain(ref, sem):
        pltpu.make_async_copy(ref, ref, sem).wait()

    def send_first(b):
        for to in peers + [me]:
            remote(s1.at[b, to], x1.at[b, me], s1s.at[b], s1r.at[b], {"row": to, "col": sib}).start()

    def gates(b):
        t = tokv[b, pl.ds(pl.multiple_of(col * span, span), span), :].astype(jnp.float32)
        scale = lax.rsqrt(jnp.mean(t * t, axis=-1, keepdims=True) + norm_eps)
        normed = (t * scale * gain[...]).astype(jnp.bfloat16)
        g = jnp.dot(normed, wg[...], preferred_element_type=jnp.float32)
        gate[b] = 0.5 * jnp.tanh(0.5 * g) + 0.5

    def transform(b):
        x = x1[b].reshape(n1, 2 * n2)
        g = jnp.dot(f1[...], x, preferred_element_type=jnp.float32)
        cos, sin = tw[0], tw[1]
        for c in range(2):
            gc = g[:n1, c * n2:(c + 1) * n2]
            gs = g[n1:, c * n2:(c + 1) * n2]
            tt[:, 2 * c * n2:(2 * c + 1) * n2] = (gc * cos - gs * sin).astype(jnp.bfloat16)
            tt[:, (2 * c + 1) * n2:(2 * c + 2) * n2] = (-(gc * sin + gs * cos)).astype(jnp.bfloat16)
        own = jnp.where(me == 0, 1, 0)

        def half(which):
            o = lax.dot_general(
                f2[own], tt[pl.ds(pl.multiple_of(which * span, span), span), :],
                (((1,), (1,)), ((), ())), preferred_element_type=jnp.float32,
            )
            return o.astype(jnp.bfloat16).reshape(rows * cols // 2, 2, span)

        xs[b] = half(core)
        swap(b).start()
        ps[b, :, core] = half(1 - core)

    def swap(b):
        return remote(
            xs.at[b], ps.at[b, :, core], sws.at[b], swr.at[b], {"col": sib}
        )

    def send_second(b):
        def one(to, c):
            remote(
                ps.at[b, lax.div(c, 2) * rows + to], spec.at[b, me, lax.div(col, 2)],
                s2s.at[b], s2r.at[b], {"row": to, "col": c},
            ).start()

        for c in across + [sib]:
            for to in peers + [me]:
                one(to, c)

    def share(owner, at, to):
        part = wo.at[:, lane_block(owner, width)]
        return remote(part, part, wos.at[at], wor.at[at], {"col": to})

    def quarter(owner, at_y, at, to):
        size = wo.shape[0] // 4
        part = wo.at[pl.ds(pl.multiple_of(at_y * size, size), size), lane_block(owner, width)]
        return remote(part, part, wos.at[at], wor.at[at], to)

    def mix(b):
        lhs = spec[b].reshape(2 * rows * cols, span)
        pre = lax.dot_general(
            lhs, ws[...], (((0,), (0,)), ((), ())), preferred_element_type=jnp.float32
        )
        return (gate[b] * pre).astype(jnp.bfloat16)

    def emit(b, mixed):
        for step in range(cols // 2):
            chip = lax.rem(lax.div(col, 2) + (2, 1, 3, 0)[step], cols // 2)
            res = jnp.dot(
                mixed, wo[:, lane_block(chip, 2 * width)], preferred_element_type=jnp.float32
            ).astype(jnp.bfloat16)
            for core in range(2):
                osc[b, chip * 2 + core] = res[:, core * width:(core + 1) * width]
            rest = pl.ds(pl.multiple_of(col * span, span), span)
            targets = (far, near[0::2], near[1::2], [sib])[step]
            for to in targets:
                remote(
                    osc.at[b, to], out.at[b, rest, :], oss.at[b], osr.at[b], {"col": to}
                ).start()
            if step == cols // 2 - 1:
                out[b, rest, :] = osc[b, col]

    scope = jax.named_scope
    with scope("project0"):
        project(0)
    with scope("barrier"):
        pl.semaphore_wait(barrier, rows - 1 + len(turns) + cols - 1)
    with scope("send0"):
        send_first(0)
    wo_load.wait()
    quarter(col, y, 7, {"col": far[0]}).start()
    share(col, 0, near[0]).start()
    share(col, 1, near[1]).start()
    share(col, 3, sib).start()
    with scope("gates"):
        wg_load.wait()
        gates(0)
    with scope("spectrum_rows"):
        spec_load.wait()
        perm_load.wait()
        ws[...] = jnp.dot(
            perm[...], wsv[...], preferred_element_type=jnp.float32
        ).astype(jnp.bfloat16)
        f1_load.wait()
        tw_load.wait()
        f2_load.wait()
    for b in range(1, batches):
        with scope("project%d" % b):
            project(b)
        with scope("send%d" % b):
            send_first(b)
        with scope("gates"):
            gates(b)
    with scope("turn"):
        quarter(far[0], y, 7, {"col": sib}).wait_recv()
        for d in (2, 1, 3):
            quarter(far[0], y, 7 + d, {"row": turns[d - 1]}).start()
    for b in range(batches):
        with scope("wait_first%d" % b):
            drain(s1.at[b], s1r.at[b])
        with scope("transform%d" % b):
            transform(b)
        with scope("swap%d" % b):
            swap(b).wait_recv()
        with scope("second%d" % b):
            send_second(b)
        if b == 0:
            with scope("share"):
                share(near[1], 0, sib).wait_recv()
                share(near[1], 4, sib).start()
                share(near[0], 1, sib).wait_recv()
                share(near[0], 5, sib).start()
    with scope("share2"):
        for d in range(1, 4):
            quarter(far[0], y, 7 + d, {"row": turns[d - 1]}).wait_recv()
        share(far[0], 2, sib).start()
        for at in range(2, 6):
            share(col, at, sib).wait_recv()
    for b in range(batches):
        with scope("wait_second%d" % b):
            drain(ps.at[b], s2r.at[b])
        with scope("mix%d" % b):
            mixed = mix(b)
        with scope("emit%d" % b):
            emit(b, mixed)
    with scope("wait_out"):
        for b in range(batches):
            drain(osc.at[b, pl.ds(0, cols - 1)], osr.at[b])
    with scope("tail"):
        for b in range(batches):
            drain(s1.at[b], s1s.at[b])
            drain(ps.at[b], s2s.at[b])
            swap(b).wait_send()
            drain(osc.at[b, pl.ds(0, cols - 1)], oss.at[b])
        for at in range(6):
            share(col, at, sib).wait_send()
        for at in range(7, 11):
            quarter(col, y, at, {"col": sib}).wait_send()


def fused(rows, cols, tokens, norm_gain, w_fourier_in, w_gate, w_spectrum, w_output):
    batches, seq_local, features = tokens.shape
    n2 = LANES
    n1 = seq_local * rows // n2
    blocks = seq_local // n2
    span = seq_local // cols
    width = w_output.shape[1]
    fold = fold_table()
    fold_high = fold.astype(jnp.bfloat16)
    fold_low = (fold - fold_high.astype(np.float64)).astype(jnp.bfloat16)
    tables = (
        jnp.asarray(np.stack([fold_high, fold_low])),
        jnp.asarray(first_table(n1), jnp.bfloat16),
        jnp.asarray(second_table(rows, n2), jnp.bfloat16),
        jnp.asarray(twist_table(n1, n2), jnp.float32),
        jnp.asarray(channel_order(rows, cols), jnp.bfloat16),
    )
    hbm = pl.BlockSpec(memory_space=pltpu.HBM)
    dma = pltpu.SemaphoreType.DMA
    half = jnp.bfloat16
    scratch = [
        (tokens.shape, half), ((1, features), jnp.float32), (w_fourier_in.shape[::-1], half),
        (w_gate.shape, half), (w_spectrum.shape, half), (w_spectrum.shape, half),
        ((features, features), half), *((t.shape, t.dtype) for t in tables),
        ((GROUP_WIDTH, features), half), ((batches, span, features), jnp.float32),
        ((GROUP_WIDTH * blocks, n2), jnp.float32), ((n1, 4 * n2), half),
        ((batches, rows, blocks, 2 * n2), half), ((batches, rows, blocks, 2 * n2), half),
        ((batches, cols // 2 * rows, 2, span), half),
        ((batches, cols // 2 * rows, 2, 2, span), half),
        ((batches, rows, cols // 2, 2, 2, span), half),
        ((batches, cols, span, width), half),
    ]
    return pl.pallas_call(
        functools.partial(mixer_kernel, rows, cols),
        out_shape=pltpu.VMEM((batches, seq_local, width), jnp.bfloat16),
        in_specs=[hbm] * 11,
        out_specs=pl.BlockSpec(memory_space=pltpu.VMEM),
        scratch_shapes=[pltpu.VMEM(shape, dtype) for shape, dtype in scratch] + [
            dma((batches, seq_local // 512)), dma((10,)),
            *(dma((batches,)) for _ in range(8)), dma((11,)), dma((11,)),
        ],
        compiler_params=pltpu.CompilerParams(
            collective_id=0, has_side_effects=True, vmem_limit_bytes=62 * 1024 * 1024
        ),
    )(tokens, norm_gain[None, :], w_fourier_in.T, w_gate, w_spectrum, w_output, *tables)


def body(rows, cols, *args):
    tokens, w_fourier_in, w_output = args[0], args[2], args[5]
    fits = (
        rows == HALF and cols == 8 and w_fourier_in.shape[1] == GROUP_WIDTH
        and tokens.shape[1:] == (16 * LANES, 8 * LANES) and w_output.shape[1] == LANES
    )
    if fits:
        return fused(rows, cols, *args)
    return on_device(*args)


def solution(mesh):
    placed = (P(None, "row", None), P(), P(None, "col"), P(), P(), P(None, "col"))
    return jax.shard_map(
        functools.partial(body, mesh.shape["row"], mesh.shape["col"]),
        mesh=mesh, in_specs=placed, out_specs=P(None, "row", "col"), check_vma=False,
    )
```

```python
import functools

import jax
import jax.numpy as jnp
import numpy as np
from jax import lax
from jax.experimental import pallas as pl
from jax.experimental.pallas import tpu as pltpu
from jax.sharding import PartitionSpec as P

GROUP_WIDTH = 64
FIRST_LEN = 256
LANES = 128


norm_eps = 1e-06


def shortened(value):
    return jax.tree.map(lambda a: a.astype(jnp.bfloat16) if a.dtype == jnp.float32 else a, value)


def over_all(value, axis, dim, absorb, carry):
    whole = jax.tree.map(lambda part: lax.all_gather(part, axis, axis=dim, tiled=True), value)
    return absorb(carry, whole, jnp.int32(0))


def dft_tables(length_in, length_out, period):
    left_index = lax.broadcasted_iota(jnp.int32, (length_in, length_out), 0)
    right_index = lax.broadcasted_iota(jnp.int32, (length_in, length_out), 1)
    angles = (left_index * right_index % period).astype(jnp.float32) * (2.0 * jnp.pi / period)
    return (jnp.cos(angles), jnp.sin(angles))


def transform_first(cube, table):
    return jnp.einsum("cpq,pk->ckq", cube, table, precision=lax.Precision.HIGHEST)


def transform_second(cube, table):
    return jnp.einsum("ckq,qj->cjk", cube, table, precision=lax.Precision.HIGHEST)


def positional(real_part, imag_part):
    rows_count, seq_total = real_part.shape
    second_len = seq_total // FIRST_LEN
    cos_first, sin_first = dft_tables(FIRST_LEN, FIRST_LEN, FIRST_LEN)
    cos_twist, sin_twist = dft_tables(FIRST_LEN, second_len, seq_total)
    cos_second, sin_second = dft_tables(second_len, second_len, second_len)
    real_cube = real_part.reshape(rows_count, FIRST_LEN, second_len)
    imag_cube = imag_part.reshape(rows_count, FIRST_LEN, second_len)
    section_real = transform_first(real_cube, cos_first) + transform_first(imag_cube, sin_first)
    section_imag = transform_first(imag_cube, cos_first) - transform_first(real_cube, sin_first)
    twist_real = section_real * cos_twist + section_imag * sin_twist
    twist_imag = section_imag * cos_twist - section_real * sin_twist
    summed = transform_second(twist_real, cos_second) + transform_second(twist_imag, sin_second)
    norm_scale = 1.0 / jnp.sqrt(jnp.float32(seq_total * GROUP_WIDTH))
    return (summed.reshape(rows_count, seq_total) * norm_scale).astype(jnp.bfloat16)


def on_device(tokens, norm_gain, w_fourier_in, w_gate, w_spectrum, w_output):
    batches, seq_local, features = tokens.shape
    tokens_count = batches * seq_local
    widened = tokens.astype(jnp.float32)
    inverse = lax.rsqrt(jnp.mean(widened * widened, axis=-1, keepdims=True) + norm_eps)
    normed = (widened * inverse * norm_gain).astype(jnp.bfloat16).reshape(tokens_count, features)
    fourier_in = jnp.dot(normed, w_fourier_in, preferred_element_type=jnp.float32).astype(
        jnp.bfloat16
    )
    local_groups = w_fourier_in.shape[1] // GROUP_WIDTH
    grouped = fourier_in.astype(jnp.float32).reshape(batches, seq_local, local_groups, GROUP_WIDTH)
    cos_group, sin_group = dft_tables(GROUP_WIDTH, GROUP_WIDTH, GROUP_WIDTH)
    real_part = jnp.einsum(
        "btgn,nm->bgmt", grouped, cos_group, precision=lax.Precision.HIGHEST
    ).reshape(-1, seq_local)
    imag_part = -jnp.einsum(
        "btgn,nm->bgmt", grouped, sin_group, precision=lax.Precision.HIGHEST
    ).reshape(-1, seq_local)
    real_part = lax.all_to_all(
        shortened(real_part), "row", split_axis=0, concat_axis=1, tiled=True
    ).astype(real_part.dtype)
    imag_part = lax.all_to_all(
        shortened(imag_part), "row", split_axis=0, concat_axis=1, tiled=True
    ).astype(imag_part.dtype)
    spectrum = positional(real_part, imag_part)
    spectrum = lax.all_to_all(spectrum, "row", split_axis=1, concat_axis=0, tiled=True)
    spectrum = spectrum.reshape(batches, local_groups * GROUP_WIDTH, seq_local)
    spectrum = jnp.transpose(spectrum, (0, 2, 1)).reshape(tokens_count, local_groups * GROUP_WIDTH)

    def add_spectrum(running, portion, beginning):
        weight_rows = lax.dynamic_slice_in_dim(w_spectrum, beginning, portion.shape[1], 0)
        return running + jnp.dot(portion, weight_rows, preferred_element_type=jnp.float32)

    mixed_pre = over_all(
        spectrum, "col", 1, add_spectrum, jnp.zeros((tokens_count, features), jnp.float32)
    ).astype(jnp.bfloat16)
    gate_pre = jnp.dot(normed, w_gate, preferred_element_type=jnp.float32)
    mixed = (jax.nn.sigmoid(gate_pre) * mixed_pre.astype(jnp.float32)).astype(jnp.bfloat16)
    result = jnp.dot(mixed, w_output, preferred_element_type=jnp.float32)
    return result.astype(jnp.bfloat16).reshape(batches, seq_local, -1)


MESH = pl.DeviceIdType.MESH
HALF = GROUP_WIDTH // 2


def fold_table():
    n = np.arange(GROUP_WIDTH)
    table = np.zeros((2, HALF, GROUP_WIDTH))
    for m in range(HALF):
        table[0, m] = np.cos(2 * np.pi * (n * m % GROUP_WIDTH) / GROUP_WIDTH)
        table[1, m] = np.sin(2 * np.pi * (n * m % GROUP_WIDTH) / GROUP_WIDTH)
    table[1, 0] = np.cos(np.pi * n)
    return table.reshape(GROUP_WIDTH, GROUP_WIDTH)


def first_table(n1):
    a = np.arange(n1)
    ang = 2 * np.pi * (np.outer(a, a) % n1) / n1
    return np.concatenate([np.cos(ang), np.sin(ang)], 0)


def twist_table(n1, n2):
    phi = 2 * np.pi * np.outer(np.arange(n1), np.arange(n2)) / (n1 * n2)
    scale = 1.0 / np.sqrt(n1 * n2 * GROUP_WIDTH)
    return np.stack([np.cos(phi) * scale, np.sin(phi) * scale])


def second_table(rows, n2):
    q = np.arange(n2)
    psi = 2 * np.pi * (np.outer(q, q) % n2) / n2
    cos, sin = np.cos(psi), np.sin(psi)
    even = np.concatenate([cos, sin], 1)
    odd = np.concatenate([sin, -cos], 1)
    zero = np.zeros_like(even)
    plain = np.stack([np.concatenate([even, -odd], 1), np.concatenate([even, odd], 1)])
    first = np.stack([np.concatenate([even, zero], 1), np.concatenate([zero, even], 1)])
    both = np.stack([plain, first])
    per = n2 // rows
    both = both.reshape(2, 2, rows, per, 4 * n2).transpose(0, 3, 2, 1, 4)
    return both.reshape(2, 2 * n2, 4 * n2)


def channel_order(rows, cols):
    take = np.zeros((rows, cols, 2), np.int64)
    for r in range(rows):
        for c in range(cols):
            group = (c + 1 - 2 * (c % 2)) * GROUP_WIDTH
            take[r, c, 0] = group + r
            take[r, c, 1] = group + (HALF if r == 0 else GROUP_WIDTH - r)
    return np.eye(rows * cols * 2)[take.reshape(-1)]


def row_offsets():
    far = lambda n: sorted(range(n), key=lambda d: -min(d, n - d))
    return [(dz, dy) for dy in far(4) for dz in far(8) if dz or dy]


def mixer_kernel(
    rows, cols, tok, gain_in, wf_in, wg_in, wspec_in, wout, fold_in, f1_in, f2_in, tw_in, perm_in, out,
    tokv, gain, wf, wg, wsv, ws, wo, fold, f1, f2, tw, perm, wp, gate, ysc, tt, s1, x1, xs, ps, spec, osc,
    tsem, lsem, s1s, s1r, sws, swr, s2s, s2r, oss, osr, wos, wor, ready,
):
    batches, seq_local, features = tok.shape
    n1, n2 = tw.shape[1:]
    blocks = seq_local // n2
    span = seq_local // cols
    width = wout.shape[1]
    chunk = 512
    chunks = seq_local // chunk
    me = lax.axis_index("row")
    col = lax.axis_index("col")
    z, y = lax.div(me, 4), lax.rem(me, 4)
    sib = col + 1 - 2 * lax.rem(col, 2)
    peers = [lax.rem(z + dz, 8) * 4 + lax.rem(y + dy, 4) for dz, dy in row_offsets()]
    far = [lax.rem(col + 4, cols), lax.rem(sib + 4, cols)]
    near = [lax.rem(col + 2, cols), lax.rem(col + 6, cols), lax.rem(sib + 2, cols), lax.rem(sib + 6, cols)]
    others = far + near + [sib]
    across = [far[1], near[2], near[3]]
    core = lax.rem(col, 2)

    line = [lax.rem(z + dz, 8) * 4 + y for dz, dy in row_offsets() if dy == 0]
    aside = [lax.rem(z + dz, 8) * 4 + lax.rem(y + dy, 4) for dz, dy in row_offsets() if dy]
    turns = [z * 4 + lax.rem(y + d, 4) for d in range(1, 4)]

    def load(src, dst, at):
        copy = pltpu.make_async_copy(src, dst, lsem.at[at])
        copy.start()
        return copy

    def lane_block(c, size):
        return pl.ds(pl.multiple_of(c * size, size), size)

    barrier = pltpu.get_barrier_semaphore()
    for to in line:
        pl.semaphore_signal(
            barrier, inc=1, device_id={"row": to, "col": sib}, device_id_type=MESH
        )
    for to in turns:
        pl.semaphore_signal(barrier, inc=1, device_id={"row": to}, device_id_type=MESH)
    for to in others:
        pl.semaphore_signal(barrier, inc=1, device_id={"col": to}, device_id_type=MESH)

    fold_load = load(fold_in, fold, 0)
    wf_load = load(wf_in, wf, 1)
    gain_load = load(gain_in, gain, 2)
    loads = {}
    for b in range(batches):
        for j in range(chunks):
            part = pl.ds(j * chunk, chunk)
            loads[b, j] = pltpu.make_async_copy(tok.at[b, part], tokv.at[b, part], tsem.at[b, j])
            loads[b, j].start()
    wo_load = load(wout, wo.at[:, lane_block(col, width)], 3)
    wg_load = load(wg_in, wg, 4)
    spec_load = load(wspec_in, wsv, 5)
    perm_load = load(perm_in, perm, 6)
    f1_load = load(f1_in, f1, 7)
    tw_load = load(tw_in, tw, 8)
    f2_load = load(f2_in, f2, 9)

    fold_load.wait()
    wf_load.wait()
    gain_load.wait()
    folded = jnp.zeros((GROUP_WIDTH, features), jnp.float32)
    for half in range(2):
        folded += lax.dot_general(
            fold[half], wf[...], (((1,), (0,)), ((), ())), preferred_element_type=jnp.float32
        )
    wp[...] = (folded * gain[...]).astype(jnp.bfloat16)

    def project(b):
        for j in range(chunks):
            loads[b, j].wait()
            t = tokv[b, j * chunk:(j + 1) * chunk, :]
            part = lax.dot_general(
                wp[...], t, (((1,), (1,)), ((), ())), preferred_element_type=jnp.float32
            )
            squares = jnp.zeros((chunk, LANES), jnp.float32)
            for k in range(features // LANES):
                w = t[:, k * LANES:(k + 1) * LANES].astype(jnp.float32)
                squares += w * w
            total = jnp.sum(squares.T, axis=0, keepdims=True)
            part = part * lax.rsqrt(total * (1.0 / features) + norm_eps)
            for k in range(chunk // n2):
                ysc[pl.ds(j * (chunk // n2) + k, GROUP_WIDTH, stride=blocks), :] = part[:, k * n2:(k + 1) * n2]
        for c in range(2):
            half = ysc[c * rows * blocks:(c + 1) * rows * blocks, :].reshape(rows, blocks, n2)
            s1[b, :, :, c * n2:(c + 1) * n2] = half.astype(jnp.bfloat16)

    def remote(src, dst, send, recv, to):
        return pltpu.make_async_remote_copy(
            src_ref=src, dst_ref=dst, send_sem=send, recv_sem=recv, device_id=to, device_id_type=MESH
        )

    def drain(ref, sem):
        pltpu.make_async_copy(ref, ref, sem).wait()

    def send_first(b, targets):
        for to in targets:
            remote(s1.at[b, to], x1.at[b, me], s1s.at[b], s1r.at[b], {"row": to, "col": sib}).start()

    def gates(b):
        t = tokv[b, pl.ds(pl.multiple_of(col * span, span), span), :].astype(jnp.float32)
        scale = lax.rsqrt(jnp.mean(t * t, axis=-1, keepdims=True) + norm_eps)
        normed = (t * scale * gain[...]).astype(jnp.bfloat16)
        g = jnp.dot(normed, wg[...], preferred_element_type=jnp.float32)
        gate[b] = 0.5 * jnp.tanh(0.5 * g) + 0.5

    def transform(b):
        x = x1[b].reshape(n1, 2 * n2)
        g = jnp.dot(f1[...], x, preferred_element_type=jnp.float32)
        cos, sin = tw[0], tw[1]
        for c in range(2):
            gc = g[:n1, c * n2:(c + 1) * n2]
            gs = g[n1:, c * n2:(c + 1) * n2]
            tt[:, 2 * c * n2:(2 * c + 1) * n2] = (gc * cos - gs * sin).astype(jnp.bfloat16)
            tt[:, (2 * c + 1) * n2:(2 * c + 2) * n2] = (-(gc * sin + gs * cos)).astype(jnp.bfloat16)
        own = jnp.where(me == 0, 1, 0)

        def half(which):
            o = lax.dot_general(
                f2[own], tt[pl.ds(pl.multiple_of(which * span, span), span), :],
                (((1,), (1,)), ((), ())), preferred_element_type=jnp.float32,
            )
            return o.astype(jnp.bfloat16).reshape(rows * cols // 2, 2, span)

        xs[b] = half(core)
        swap(b).start()
        ps[b, :, core] = half(1 - core)

    def swap(b):
        return remote(
            xs.at[b], ps.at[b, :, core], sws.at[b], swr.at[b], {"col": sib}
        )

    def send_second(b):
        def one(to, c):
            remote(
                ps.at[b, lax.div(c, 2) * rows + to], spec.at[b, me, lax.div(col, 2)],
                s2s.at[b], s2r.at[b], {"row": to, "col": c},
            ).start()

        for c in across + [sib]:
            for to in peers + [me]:
                one(to, c)

    def share(owner, at, to):
        part = wo.at[:, lane_block(owner, width)]
        return remote(part, part, wos.at[at], wor.at[at], {"col": to})

    def quarter(owner, at_y, at, to):
        size = wo.shape[0] // 4
        part = wo.at[pl.ds(pl.multiple_of(at_y * size, size), size), lane_block(owner, width)]
        return remote(part, part, wos.at[at], wor.at[at], to)

    def mix(b):
        lhs = spec[b].reshape(2 * rows * cols, span)
        pre = lax.dot_general(
            lhs, ws[...], (((0,), (0,)), ((), ())), preferred_element_type=jnp.float32
        )
        return (gate[b] * pre).astype(jnp.bfloat16)

    def emit(b, mixed):
        for step in range(cols // 2):
            chip = lax.rem(lax.div(col, 2) + (2, 1, 3, 0)[step], cols // 2)
            res = jnp.dot(
                mixed, wo[:, lane_block(chip, 2 * width)], preferred_element_type=jnp.float32
            ).astype(jnp.bfloat16)
            for core in range(2):
                osc[b, chip * 2 + core] = res[:, core * width:(core + 1) * width]
            rest = pl.ds(pl.multiple_of(col * span, span), span)
            targets = (far, near[0::2], near[1::2], [sib])[step]
            for to in targets:
                remote(
                    osc.at[b, to], out.at[b, rest, :], oss.at[b], osr.at[b], {"col": to}
                ).start()
            if step == cols // 2 - 1:
                out[b, rest, :] = osc[b, col]

    scope = jax.named_scope
    with scope("project0"):
        project(0)
    with scope("barrier"):
        pl.semaphore_wait(barrier, len(line) + len(turns) + cols - 1)
    for to in turns:
        pl.semaphore_signal(ready, inc=1, device_id={"row": to}, device_id_type=MESH)
    with scope("send0"):
        send_first(0, line)
    with scope("ready"):
        pl.semaphore_wait(ready, len(turns))
    with scope("send0b"):
        send_first(0, aside + [me])
    wo_load.wait()
    quarter(col, y, 7, {"col": far[0]}).start()
    share(col, 0, near[0]).start()
    share(col, 1, near[1]).start()
    share(col, 3, sib).start()
    for b in range(1, batches):
        with scope("project%d" % b):
            project(b)
        with scope("send%d" % b):
            send_first(b, peers + [me])
    with scope("gates"):
        wg_load.wait()
        gates(0)
    with scope("spectrum_rows"):
        spec_load.wait()
        perm_load.wait()
        ws[...] = jnp.dot(
            perm[...], wsv[...], preferred_element_type=jnp.float32
        ).astype(jnp.bfloat16)
        f1_load.wait()
        tw_load.wait()
        f2_load.wait()
    with scope("gates"):
        for b in range(1, batches):
            gates(b)
    with scope("turn"):
        quarter(far[0], y, 7, {"col": sib}).wait_recv()
        for d in (2, 1, 3):
            quarter(far[0], y, 7 + d, {"row": turns[d - 1]}).start()
    for b in range(batches):
        with scope("wait_first%d" % b):
            drain(s1.at[b], s1r.at[b])
        with scope("transform%d" % b):
            transform(b)
        with scope("swap%d" % b):
            swap(b).wait_recv()
        with scope("second%d" % b):
            send_second(b)
        if b == 0:
            with scope("share"):
                share(near[1], 0, sib).wait_recv()
                share(near[1], 4, sib).start()
                share(near[0], 1, sib).wait_recv()
                share(near[0], 5, sib).start()
    with scope("share2"):
        for d in range(1, 4):
            quarter(far[0], y, 7 + d, {"row": turns[d - 1]}).wait_recv()
        share(far[0], 2, sib).start()
        for at in range(2, 6):
            share(col, at, sib).wait_recv()
    for b in range(batches):
        with scope("wait_second%d" % b):
            drain(ps.at[b], s2r.at[b])
        with scope("mix%d" % b):
            mixed = mix(b)
        with scope("emit%d" % b):
            emit(b, mixed)
    with scope("wait_out"):
        for b in range(batches):
            drain(osc.at[b, pl.ds(0, cols - 1)], osr.at[b])
    with scope("tail"):
        for b in range(batches):
            drain(s1.at[b], s1s.at[b])
            drain(ps.at[b], s2s.at[b])
            swap(b).wait_send()
            drain(osc.at[b, pl.ds(0, cols - 1)], oss.at[b])
        for at in range(6):
            share(col, at, sib).wait_send()
        for at in range(7, 11):
            quarter(col, y, at, {"col": sib}).wait_send()


def fused(rows, cols, tokens, norm_gain, w_fourier_in, w_gate, w_spectrum, w_output):
    batches, seq_local, features = tokens.shape
    n2 = LANES
    n1 = seq_local * rows // n2
    blocks = seq_local // n2
    span = seq_local // cols
    width = w_output.shape[1]
    fold = fold_table()
    fold_high = fold.astype(jnp.bfloat16)
    fold_low = (fold - fold_high.astype(np.float64)).astype(jnp.bfloat16)
    tables = (
        jnp.asarray(np.stack([fold_high, fold_low])),
        jnp.asarray(first_table(n1), jnp.bfloat16),
        jnp.asarray(second_table(rows, n2), jnp.bfloat16),
        jnp.asarray(twist_table(n1, n2), jnp.float32),
        jnp.asarray(channel_order(rows, cols), jnp.bfloat16),
    )
    hbm = pl.BlockSpec(memory_space=pltpu.HBM)
    dma = pltpu.SemaphoreType.DMA
    half = jnp.bfloat16
    scratch = [
        (tokens.shape, half), ((1, features), jnp.float32), (w_fourier_in.shape[::-1], half),
        (w_gate.shape, half), (w_spectrum.shape, half), (w_spectrum.shape, half),
        ((features, features), half), *((t.shape, t.dtype) for t in tables),
        ((GROUP_WIDTH, features), half), ((batches, span, features), jnp.float32),
        ((GROUP_WIDTH * blocks, n2), jnp.float32), ((n1, 4 * n2), half),
        ((batches, rows, blocks, 2 * n2), half), ((batches, rows, blocks, 2 * n2), half),
        ((batches, cols // 2 * rows, 2, span), half),
        ((batches, cols // 2 * rows, 2, 2, span), half),
        ((batches, rows, cols // 2, 2, 2, span), half),
        ((batches, cols, span, width), half),
    ]
    return pl.pallas_call(
        functools.partial(mixer_kernel, rows, cols),
        out_shape=pltpu.VMEM((batches, seq_local, width), jnp.bfloat16),
        in_specs=[hbm] * 11,
        out_specs=pl.BlockSpec(memory_space=pltpu.VMEM),
        scratch_shapes=[pltpu.VMEM(shape, dtype) for shape, dtype in scratch] + [
            dma((batches, seq_local // 512)), dma((10,)),
            *(dma((batches,)) for _ in range(8)), dma((11,)), dma((11,)), pltpu.SemaphoreType.REGULAR,
        ],
        compiler_params=pltpu.CompilerParams(
            collective_id=0, has_side_effects=True, vmem_limit_bytes=62 * 1024 * 1024
        ),
    )(tokens, norm_gain[None, :], w_fourier_in.T, w_gate, w_spectrum, w_output, *tables)


def body(rows, cols, *args):
    tokens, w_fourier_in, w_output = args[0], args[2], args[5]
    fits = (
        rows == HALF and cols == 8 and w_fourier_in.shape[1] == GROUP_WIDTH
        and tokens.shape[1:] == (16 * LANES, 8 * LANES) and w_output.shape[1] == LANES
    )
    if fits:
        return fused(rows, cols, *args)
    return on_device(*args)


def solution(mesh):
    placed = (P(None, "row", None), P(), P(None, "col"), P(), P(), P(None, "col"))
    return jax.shard_map(
        functools.partial(body, mesh.shape["row"], mesh.shape["col"]),
        mesh=mesh, in_specs=placed, out_specs=P(None, "row", "col"), check_vma=False,
    )
```

```python
import functools

import jax
import jax.numpy as jnp
import numpy as np
from jax import lax
from jax.experimental import pallas as pl
from jax.experimental.pallas import tpu as pltpu
from jax.sharding import PartitionSpec as P

GROUP_WIDTH = 64
FIRST_LEN = 256
LANES = 128


norm_eps = 1e-06


def shortened(value):
    return jax.tree.map(lambda a: a.astype(jnp.bfloat16) if a.dtype == jnp.float32 else a, value)


def over_all(value, axis, dim, absorb, carry):
    whole = jax.tree.map(lambda part: lax.all_gather(part, axis, axis=dim, tiled=True), value)
    return absorb(carry, whole, jnp.int32(0))


def dft_tables(length_in, length_out, period):
    left_index = lax.broadcasted_iota(jnp.int32, (length_in, length_out), 0)
    right_index = lax.broadcasted_iota(jnp.int32, (length_in, length_out), 1)
    angles = (left_index * right_index % period).astype(jnp.float32) * (2.0 * jnp.pi / period)
    return (jnp.cos(angles), jnp.sin(angles))


def transform_first(cube, table):
    return jnp.einsum("cpq,pk->ckq", cube, table, precision=lax.Precision.HIGHEST)


def transform_second(cube, table):
    return jnp.einsum("ckq,qj->cjk", cube, table, precision=lax.Precision.HIGHEST)


def positional(real_part, imag_part):
    rows_count, seq_total = real_part.shape
    second_len = seq_total // FIRST_LEN
    cos_first, sin_first = dft_tables(FIRST_LEN, FIRST_LEN, FIRST_LEN)
    cos_twist, sin_twist = dft_tables(FIRST_LEN, second_len, seq_total)
    cos_second, sin_second = dft_tables(second_len, second_len, second_len)
    real_cube = real_part.reshape(rows_count, FIRST_LEN, second_len)
    imag_cube = imag_part.reshape(rows_count, FIRST_LEN, second_len)
    section_real = transform_first(real_cube, cos_first) + transform_first(imag_cube, sin_first)
    section_imag = transform_first(imag_cube, cos_first) - transform_first(real_cube, sin_first)
    twist_real = section_real * cos_twist + section_imag * sin_twist
    twist_imag = section_imag * cos_twist - section_real * sin_twist
    summed = transform_second(twist_real, cos_second) + transform_second(twist_imag, sin_second)
    norm_scale = 1.0 / jnp.sqrt(jnp.float32(seq_total * GROUP_WIDTH))
    return (summed.reshape(rows_count, seq_total) * norm_scale).astype(jnp.bfloat16)


def on_device(tokens, norm_gain, w_fourier_in, w_gate, w_spectrum, w_output):
    batches, seq_local, features = tokens.shape
    tokens_count = batches * seq_local
    widened = tokens.astype(jnp.float32)
    inverse = lax.rsqrt(jnp.mean(widened * widened, axis=-1, keepdims=True) + norm_eps)
    normed = (widened * inverse * norm_gain).astype(jnp.bfloat16).reshape(tokens_count, features)
    fourier_in = jnp.dot(normed, w_fourier_in, preferred_element_type=jnp.float32).astype(
        jnp.bfloat16
    )
    local_groups = w_fourier_in.shape[1] // GROUP_WIDTH
    grouped = fourier_in.astype(jnp.float32).reshape(batches, seq_local, local_groups, GROUP_WIDTH)
    cos_group, sin_group = dft_tables(GROUP_WIDTH, GROUP_WIDTH, GROUP_WIDTH)
    real_part = jnp.einsum(
        "btgn,nm->bgmt", grouped, cos_group, precision=lax.Precision.HIGHEST
    ).reshape(-1, seq_local)
    imag_part = -jnp.einsum(
        "btgn,nm->bgmt", grouped, sin_group, precision=lax.Precision.HIGHEST
    ).reshape(-1, seq_local)
    real_part = lax.all_to_all(
        shortened(real_part), "row", split_axis=0, concat_axis=1, tiled=True
    ).astype(real_part.dtype)
    imag_part = lax.all_to_all(
        shortened(imag_part), "row", split_axis=0, concat_axis=1, tiled=True
    ).astype(imag_part.dtype)
    spectrum = positional(real_part, imag_part)
    spectrum = lax.all_to_all(spectrum, "row", split_axis=1, concat_axis=0, tiled=True)
    spectrum = spectrum.reshape(batches, local_groups * GROUP_WIDTH, seq_local)
    spectrum = jnp.transpose(spectrum, (0, 2, 1)).reshape(tokens_count, local_groups * GROUP_WIDTH)

    def add_spectrum(running, portion, beginning):
        weight_rows = lax.dynamic_slice_in_dim(w_spectrum, beginning, portion.shape[1], 0)
        return running + jnp.dot(portion, weight_rows, preferred_element_type=jnp.float32)

    mixed_pre = over_all(
        spectrum, "col", 1, add_spectrum, jnp.zeros((tokens_count, features), jnp.float32)
    ).astype(jnp.bfloat16)
    gate_pre = jnp.dot(normed, w_gate, preferred_element_type=jnp.float32)
    mixed = (jax.nn.sigmoid(gate_pre) * mixed_pre.astype(jnp.float32)).astype(jnp.bfloat16)
    result = jnp.dot(mixed, w_output, preferred_element_type=jnp.float32)
    return result.astype(jnp.bfloat16).reshape(batches, seq_local, -1)


MESH = pl.DeviceIdType.MESH
HALF = GROUP_WIDTH // 2


def fold_table():
    n = np.arange(GROUP_WIDTH)
    table = np.zeros((2, HALF, GROUP_WIDTH))
    for m in range(HALF):
        table[0, m] = np.cos(2 * np.pi * (n * m % GROUP_WIDTH) / GROUP_WIDTH)
        table[1, m] = np.sin(2 * np.pi * (n * m % GROUP_WIDTH) / GROUP_WIDTH)
    table[1, 0] = np.cos(np.pi * n)
    return table.reshape(GROUP_WIDTH, GROUP_WIDTH)


def first_table(n1):
    a = np.arange(n1)
    ang = 2 * np.pi * (np.outer(a, a) % n1) / n1
    return np.concatenate([np.cos(ang), np.sin(ang)], 0)


def twist_table(n1, n2):
    phi = 2 * np.pi * np.outer(np.arange(n1), np.arange(n2)) / (n1 * n2)
    scale = 1.0 / np.sqrt(n1 * n2 * GROUP_WIDTH)
    return np.stack([np.cos(phi) * scale, np.sin(phi) * scale])


def second_table(rows, n2):
    q = np.arange(n2)
    psi = 2 * np.pi * (np.outer(q, q) % n2) / n2
    cos, sin = np.cos(psi), np.sin(psi)
    even = np.concatenate([cos, sin], 1)
    odd = np.concatenate([sin, -cos], 1)
    zero = np.zeros_like(even)
    plain = np.stack([np.concatenate([even, -odd], 1), np.concatenate([even, odd], 1)])
    first = np.stack([np.concatenate([even, zero], 1), np.concatenate([zero, even], 1)])
    both = np.stack([plain, first])
    per = n2 // rows
    both = both.reshape(2, 2, rows, per, 4 * n2).transpose(0, 3, 2, 1, 4)
    return both.reshape(2, 2 * n2, 4 * n2)


def channel_order(rows, cols):
    take = np.zeros((rows, cols, 2), np.int64)
    for r in range(rows):
        for c in range(cols):
            group = (c + 1 - 2 * (c % 2)) * GROUP_WIDTH
            take[r, c, 0] = group + r
            take[r, c, 1] = group + (HALF if r == 0 else GROUP_WIDTH - r)
    return np.eye(rows * cols * 2)[take.reshape(-1)]


def row_offsets():
    far = lambda n: sorted(range(n), key=lambda d: -min(d, n - d))
    return [(dz, dy) for dy in far(4) for dz in far(8) if dz or dy]


def mixer_kernel(
    rows, cols, tok, gain_in, wf_in, wg_in, wspec_in, wout, fold_in, f1_in, f2_in, tw_in, perm_in, out,
    tokv, gain, wf, wg, wsv, ws, wo, fold, f1, f2, tw, perm, wp, gate, ysc, tt, s1, x1, xs, ps, spec, osc,
    tsem, lsem, s1s, s1r, sws, swr, s2s, s2r, oss, osr, wos, wor, ready,
):
    batches, seq_local, features = tok.shape
    n1, n2 = tw.shape[1:]
    blocks = seq_local // n2
    span = seq_local // cols
    width = wout.shape[1]
    chunk = 512
    chunks = seq_local // chunk
    me = lax.axis_index("row")
    col = lax.axis_index("col")
    z, y = lax.div(me, 4), lax.rem(me, 4)
    sib = col + 1 - 2 * lax.rem(col, 2)
    peers = [lax.rem(z + dz, 8) * 4 + lax.rem(y + dy, 4) for dz, dy in row_offsets()]
    far = [lax.rem(col + 4, cols), lax.rem(sib + 4, cols)]
    near = [lax.rem(col + 2, cols), lax.rem(col + 6, cols), lax.rem(sib + 2, cols), lax.rem(sib + 6, cols)]
    others = far + near + [sib]
    across = [far[1], near[2], near[3]]
    core = lax.rem(col, 2)

    line = [lax.rem(z + dz, 8) * 4 + y for dz, dy in row_offsets() if dy == 0]
    aside = [lax.rem(z + dz, 8) * 4 + lax.rem(y + dy, 4) for dz, dy in row_offsets() if dy]
    turns = [z * 4 + lax.rem(y + d, 4) for d in range(1, 4)]

    def load(src, dst, at):
        copy = pltpu.make_async_copy(src, dst, lsem.at[at])
        copy.start()
        return copy

    def lane_block(c, size):
        return pl.ds(pl.multiple_of(c * size, size), size)

    barrier = pltpu.get_barrier_semaphore()
    for to in line:
        pl.semaphore_signal(
            barrier, inc=1, device_id={"row": to, "col": sib}, device_id_type=MESH
        )
    for to in turns:
        pl.semaphore_signal(barrier, inc=1, device_id={"row": to}, device_id_type=MESH)
    for to in others:
        pl.semaphore_signal(barrier, inc=1, device_id={"col": to}, device_id_type=MESH)

    fold_load = load(fold_in, fold, 0)
    wf_load = load(wf_in, wf, 1)
    gain_load = load(gain_in, gain, 2)
    loads = {}
    for b in range(batches):
        for j in range(chunks):
            part = pl.ds(j * chunk, chunk)
            loads[b, j] = pltpu.make_async_copy(tok.at[b, part], tokv.at[b, part], tsem.at[b, j])
            loads[b, j].start()
    wo_load = load(wout, wo.at[:, lane_block(col, width)], 3)
    wg_load = load(wg_in, wg, 4)
    spec_load = load(wspec_in, wsv, 5)
    perm_load = load(perm_in, perm, 6)
    f1_load = load(f1_in, f1, 7)
    tw_load = load(tw_in, tw, 8)
    f2_load = load(f2_in, f2, 9)

    fold_load.wait()
    wf_load.wait()
    gain_load.wait()
    folded = jnp.zeros((GROUP_WIDTH, features), jnp.float32)
    for half in range(2):
        folded += lax.dot_general(
            fold[half], wf[...], (((1,), (0,)), ((), ())), preferred_element_type=jnp.float32
        )
    wp[...] = (folded * gain[...]).astype(jnp.bfloat16)

    def project(b):
        for j in range(chunks):
            loads[b, j].wait()
            t = tokv[b, j * chunk:(j + 1) * chunk, :]
            part = lax.dot_general(
                wp[...], t, (((1,), (1,)), ((), ())), preferred_element_type=jnp.float32
            )
            squares = jnp.zeros((chunk, LANES), jnp.float32)
            for k in range(features // LANES):
                w = t[:, k * LANES:(k + 1) * LANES].astype(jnp.float32)
                squares += w * w
            total = jnp.sum(squares.T, axis=0, keepdims=True)
            part = part * lax.rsqrt(total * (1.0 / features) + norm_eps)
            for k in range(chunk // n2):
                ysc[pl.ds(j * (chunk // n2) + k, GROUP_WIDTH, stride=blocks), :] = part[:, k * n2:(k + 1) * n2]
        for c in range(2):
            half = ysc[c * rows * blocks:(c + 1) * rows * blocks, :].reshape(rows, blocks, n2)
            s1[b, :, :, c * n2:(c + 1) * n2] = half.astype(jnp.bfloat16)

    def remote(src, dst, send, recv, to):
        return pltpu.make_async_remote_copy(
            src_ref=src, dst_ref=dst, send_sem=send, recv_sem=recv, device_id=to, device_id_type=MESH
        )

    def drain(ref, sem):
        pltpu.make_async_copy(ref, ref, sem).wait()

    def send_first(b, targets):
        for to in targets:
            remote(s1.at[b, to], x1.at[b, me], s1s.at[b], s1r.at[b], {"row": to, "col": sib}).start()

    def gates(b):
        t = tokv[b, pl.ds(pl.multiple_of(col * span, span), span), :].astype(jnp.float32)
        scale = lax.rsqrt(jnp.mean(t * t, axis=-1, keepdims=True) + norm_eps)
        normed = (t * scale * gain[...]).astype(jnp.bfloat16)
        g = jnp.dot(normed, wg[...], preferred_element_type=jnp.float32)
        gate[b] = 0.5 * jnp.tanh(0.5 * g) + 0.5

    def transform(b):
        x = x1[b].reshape(n1, 2 * n2)
        g = jnp.dot(f1[...], x, preferred_element_type=jnp.float32)
        cos, sin = tw[0], tw[1]
        for c in range(2):
            gc = g[:n1, c * n2:(c + 1) * n2]
            gs = g[n1:, c * n2:(c + 1) * n2]
            tt[:, 2 * c * n2:(2 * c + 1) * n2] = (gc * cos - gs * sin).astype(jnp.bfloat16)
            tt[:, (2 * c + 1) * n2:(2 * c + 2) * n2] = (-(gc * sin + gs * cos)).astype(jnp.bfloat16)
        own = jnp.where(me == 0, 1, 0)

        def half(which):
            o = lax.dot_general(
                f2[own], tt[pl.ds(pl.multiple_of(which * span, span), span), :],
                (((1,), (1,)), ((), ())), preferred_element_type=jnp.float32,
            )
            return o.astype(jnp.bfloat16).reshape(rows * cols // 2, 2, span)

        xs[b] = half(core)
        swap(b).start()
        ps[b, :, core] = half(1 - core)

    def swap(b):
        return remote(
            xs.at[b], ps.at[b, :, core], sws.at[b], swr.at[b], {"col": sib}
        )

    def send_second(b):
        def one(to, c):
            remote(
                ps.at[b, lax.div(c, 2) * rows + to], spec.at[b, me, lax.div(col, 2)],
                s2s.at[b], s2r.at[b], {"row": to, "col": c},
            ).start()

        for c in across + [sib]:
            for to in peers + [me]:
                one(to, c)

    def share(owner, at, to):
        part = wo.at[:, lane_block(owner, width)]
        return remote(part, part, wos.at[at], wor.at[at], {"col": to})

    def quarter(owner, at_y, at, to):
        size = wo.shape[0] // 4
        part = wo.at[pl.ds(pl.multiple_of(at_y * size, size), size), lane_block(owner, width)]
        return remote(part, part, wos.at[at], wor.at[at], to)

    def mix(b, at, size):
        lhs = spec[b, :, :, :, :, at:at + size].reshape(2 * rows * cols, size)
        pre = lax.dot_general(
            lhs, ws[...], (((0,), (0,)), ((), ())), preferred_element_type=jnp.float32
        )
        return (gate[b, at:at + size, :] * pre).astype(jnp.bfloat16)

    def emit(b, mixed, at, size, step):
        chip = lax.rem(lax.div(col, 2) + (2, 1, 3, 0)[step], cols // 2)
        res = jnp.dot(
            mixed, wo[:, lane_block(chip, 2 * width)], preferred_element_type=jnp.float32
        ).astype(jnp.bfloat16)
        for k in range(2):
            osc[b, chip * 2 + k, at:at + size, :] = res[:, k * width:(k + 1) * width]
        rest = pl.ds(pl.multiple_of(col * span + at, size), size)
        for to in (far, near[0::2], near[1::2], [sib])[step]:
            remote(
                osc.at[b, to, pl.ds(at, size)], out.at[b, rest, :], oss.at[b], osr.at[b],
                {"col": to},
            ).start()
        if step == cols // 2 - 1:
            out[b, rest, :] = osc[b, col, at:at + size, :]

    def finish(b):
        size = span // 2
        low = mix(b, 0, size)
        emit(b, low, 0, size, 0)
        high = mix(b, size, size)
        emit(b, high, size, size, 0)
        mixed = jnp.concatenate([low, high], axis=0)
        for step in range(1, cols // 2):
            emit(b, mixed, 0, span, step)

    scope = jax.named_scope
    with scope("project0"):
        project(0)
    with scope("barrier"):
        pl.semaphore_wait(barrier, len(line) + len(turns) + cols - 1)
    for to in turns:
        pl.semaphore_signal(ready, inc=1, device_id={"row": to}, device_id_type=MESH)
    with scope("send0"):
        send_first(0, line)
    with scope("ready"):
        pl.semaphore_wait(ready, len(turns))
    with scope("send0b"):
        send_first(0, aside + [me])
    wo_load.wait()
    quarter(col, y, 7, {"col": far[0]}).start()
    share(col, 0, near[0]).start()
    share(col, 1, near[1]).start()
    share(col, 3, sib).start()
    for b in range(1, batches):
        with scope("project%d" % b):
            project(b)
        with scope("send%d" % b):
            send_first(b, peers + [me])
    with scope("gates"):
        wg_load.wait()
        gates(0)
    with scope("spectrum_rows"):
        spec_load.wait()
        perm_load.wait()
        ws[...] = jnp.dot(
            perm[...], wsv[...], preferred_element_type=jnp.float32
        ).astype(jnp.bfloat16)
        f1_load.wait()
        tw_load.wait()
        f2_load.wait()
    with scope("gates"):
        for b in range(1, batches):
            gates(b)
    with scope("turn"):
        quarter(far[0], y, 7, {"col": sib}).wait_recv()
        for d in (2, 1, 3):
            quarter(far[0], y, 7 + d, {"row": turns[d - 1]}).start()
    for b in range(batches):
        with scope("wait_first%d" % b):
            drain(s1.at[b], s1r.at[b])
        with scope("transform%d" % b):
            transform(b)
        with scope("swap%d" % b):
            swap(b).wait_recv()
        with scope("second%d" % b):
            send_second(b)
        if b == 0:
            with scope("share"):
                share(near[1], 0, sib).wait_recv()
                share(near[1], 4, sib).start()
                share(near[0], 1, sib).wait_recv()
                share(near[0], 5, sib).start()
    with scope("share2"):
        for d in range(1, 4):
            quarter(far[0], y, 7 + d, {"row": turns[d - 1]}).wait_recv()
        share(far[0], 2, sib).start()
        for at in range(2, 6):
            share(col, at, sib).wait_recv()
    for b in range(batches):
        with scope("wait_second%d" % b):
            drain(ps.at[b], s2r.at[b])
        with scope("finish%d" % b):
            finish(b)
    with scope("wait_out"):
        for b in range(batches):
            drain(osc.at[b, pl.ds(0, cols - 1)], osr.at[b])
    with scope("tail"):
        for b in range(batches):
            drain(s1.at[b], s1s.at[b])
            drain(ps.at[b], s2s.at[b])
            swap(b).wait_send()
            drain(osc.at[b, pl.ds(0, cols - 1)], oss.at[b])
        for at in range(6):
            share(col, at, sib).wait_send()
        for at in range(7, 11):
            quarter(col, y, at, {"col": sib}).wait_send()


def fused(rows, cols, tokens, norm_gain, w_fourier_in, w_gate, w_spectrum, w_output):
    batches, seq_local, features = tokens.shape
    n2 = LANES
    n1 = seq_local * rows // n2
    blocks = seq_local // n2
    span = seq_local // cols
    width = w_output.shape[1]
    fold = fold_table()
    fold_high = fold.astype(jnp.bfloat16)
    fold_low = (fold - fold_high.astype(np.float64)).astype(jnp.bfloat16)
    tables = (
        jnp.asarray(np.stack([fold_high, fold_low])),
        jnp.asarray(first_table(n1), jnp.bfloat16),
        jnp.asarray(second_table(rows, n2), jnp.bfloat16),
        jnp.asarray(twist_table(n1, n2), jnp.float32),
        jnp.asarray(channel_order(rows, cols), jnp.bfloat16),
    )
    hbm = pl.BlockSpec(memory_space=pltpu.HBM)
    dma = pltpu.SemaphoreType.DMA
    half = jnp.bfloat16
    scratch = [
        (tokens.shape, half), ((1, features), jnp.float32), (w_fourier_in.shape[::-1], half),
        (w_gate.shape, half), (w_spectrum.shape, half), (w_spectrum.shape, half),
        ((features, features), half), *((t.shape, t.dtype) for t in tables),
        ((GROUP_WIDTH, features), half), ((batches, span, features), jnp.float32),
        ((GROUP_WIDTH * blocks, n2), jnp.float32), ((n1, 4 * n2), half),
        ((batches, rows, blocks, 2 * n2), half), ((batches, rows, blocks, 2 * n2), half),
        ((batches, cols // 2 * rows, 2, span), half),
        ((batches, cols // 2 * rows, 2, 2, span), half),
        ((batches, rows, cols // 2, 2, 2, span), half),
        ((batches, cols, span, width), half),
    ]
    return pl.pallas_call(
        functools.partial(mixer_kernel, rows, cols),
        out_shape=pltpu.VMEM((batches, seq_local, width), jnp.bfloat16),
        in_specs=[hbm] * 11,
        out_specs=pl.BlockSpec(memory_space=pltpu.VMEM),
        scratch_shapes=[pltpu.VMEM(shape, dtype) for shape, dtype in scratch] + [
            dma((batches, seq_local // 512)), dma((10,)),
            *(dma((batches,)) for _ in range(8)), dma((11,)), dma((11,)), pltpu.SemaphoreType.REGULAR,
        ],
        compiler_params=pltpu.CompilerParams(
            collective_id=0, has_side_effects=True, vmem_limit_bytes=62 * 1024 * 1024
        ),
    )(tokens, norm_gain[None, :], w_fourier_in.T, w_gate, w_spectrum, w_output, *tables)


def body(rows, cols, *args):
    tokens, w_fourier_in, w_output = args[0], args[2], args[5]
    fits = (
        rows == HALF and cols == 8 and w_fourier_in.shape[1] == GROUP_WIDTH
        and tokens.shape[1:] == (16 * LANES, 8 * LANES) and w_output.shape[1] == LANES
    )
    if fits:
        return fused(rows, cols, *args)
    return on_device(*args)


def solution(mesh):
    placed = (P(None, "row", None), P(), P(None, "col"), P(), P(), P(None, "col"))
    return jax.shard_map(
        functools.partial(body, mesh.shape["row"], mesh.shape["col"]),
        mesh=mesh, in_specs=placed, out_specs=P(None, "row", "col"), check_vma=False,
    )
```

```python
import functools

import jax
import jax.numpy as jnp
import numpy as np
from jax import lax
from jax.experimental import pallas as pl
from jax.experimental.pallas import tpu as pltpu
from jax.sharding import PartitionSpec as P

GROUP_WIDTH = 64
FIRST_LEN = 256
LANES = 128


norm_eps = 1e-06


def shortened(value):
    return jax.tree.map(lambda a: a.astype(jnp.bfloat16) if a.dtype == jnp.float32 else a, value)


def over_all(value, axis, dim, absorb, carry):
    whole = jax.tree.map(lambda part: lax.all_gather(part, axis, axis=dim, tiled=True), value)
    return absorb(carry, whole, jnp.int32(0))


def dft_tables(length_in, length_out, period):
    left_index = lax.broadcasted_iota(jnp.int32, (length_in, length_out), 0)
    right_index = lax.broadcasted_iota(jnp.int32, (length_in, length_out), 1)
    angles = (left_index * right_index % period).astype(jnp.float32) * (2.0 * jnp.pi / period)
    return (jnp.cos(angles), jnp.sin(angles))


def transform_first(cube, table):
    return jnp.einsum("cpq,pk->ckq", cube, table, precision=lax.Precision.HIGHEST)


def transform_second(cube, table):
    return jnp.einsum("ckq,qj->cjk", cube, table, precision=lax.Precision.HIGHEST)


def positional(real_part, imag_part):
    rows_count, seq_total = real_part.shape
    second_len = seq_total // FIRST_LEN
    cos_first, sin_first = dft_tables(FIRST_LEN, FIRST_LEN, FIRST_LEN)
    cos_twist, sin_twist = dft_tables(FIRST_LEN, second_len, seq_total)
    cos_second, sin_second = dft_tables(second_len, second_len, second_len)
    real_cube = real_part.reshape(rows_count, FIRST_LEN, second_len)
    imag_cube = imag_part.reshape(rows_count, FIRST_LEN, second_len)
    section_real = transform_first(real_cube, cos_first) + transform_first(imag_cube, sin_first)
    section_imag = transform_first(imag_cube, cos_first) - transform_first(real_cube, sin_first)
    twist_real = section_real * cos_twist + section_imag * sin_twist
    twist_imag = section_imag * cos_twist - section_real * sin_twist
    summed = transform_second(twist_real, cos_second) + transform_second(twist_imag, sin_second)
    norm_scale = 1.0 / jnp.sqrt(jnp.float32(seq_total * GROUP_WIDTH))
    return (summed.reshape(rows_count, seq_total) * norm_scale).astype(jnp.bfloat16)


def on_device(tokens, norm_gain, w_fourier_in, w_gate, w_spectrum, w_output):
    batches, seq_local, features = tokens.shape
    tokens_count = batches * seq_local
    widened = tokens.astype(jnp.float32)
    inverse = lax.rsqrt(jnp.mean(widened * widened, axis=-1, keepdims=True) + norm_eps)
    normed = (widened * inverse * norm_gain).astype(jnp.bfloat16).reshape(tokens_count, features)
    fourier_in = jnp.dot(normed, w_fourier_in, preferred_element_type=jnp.float32).astype(
        jnp.bfloat16
    )
    local_groups = w_fourier_in.shape[1] // GROUP_WIDTH
    grouped = fourier_in.astype(jnp.float32).reshape(batches, seq_local, local_groups, GROUP_WIDTH)
    cos_group, sin_group = dft_tables(GROUP_WIDTH, GROUP_WIDTH, GROUP_WIDTH)
    real_part = jnp.einsum(
        "btgn,nm->bgmt", grouped, cos_group, precision=lax.Precision.HIGHEST
    ).reshape(-1, seq_local)
    imag_part = -jnp.einsum(
        "btgn,nm->bgmt", grouped, sin_group, precision=lax.Precision.HIGHEST
    ).reshape(-1, seq_local)
    real_part = lax.all_to_all(
        shortened(real_part), "row", split_axis=0, concat_axis=1, tiled=True
    ).astype(real_part.dtype)
    imag_part = lax.all_to_all(
        shortened(imag_part), "row", split_axis=0, concat_axis=1, tiled=True
    ).astype(imag_part.dtype)
    spectrum = positional(real_part, imag_part)
    spectrum = lax.all_to_all(spectrum, "row", split_axis=1, concat_axis=0, tiled=True)
    spectrum = spectrum.reshape(batches, local_groups * GROUP_WIDTH, seq_local)
    spectrum = jnp.transpose(spectrum, (0, 2, 1)).reshape(tokens_count, local_groups * GROUP_WIDTH)

    def add_spectrum(running, portion, beginning):
        weight_rows = lax.dynamic_slice_in_dim(w_spectrum, beginning, portion.shape[1], 0)
        return running + jnp.dot(portion, weight_rows, preferred_element_type=jnp.float32)

    mixed_pre = over_all(
        spectrum, "col", 1, add_spectrum, jnp.zeros((tokens_count, features), jnp.float32)
    ).astype(jnp.bfloat16)
    gate_pre = jnp.dot(normed, w_gate, preferred_element_type=jnp.float32)
    mixed = (jax.nn.sigmoid(gate_pre) * mixed_pre.astype(jnp.float32)).astype(jnp.bfloat16)
    result = jnp.dot(mixed, w_output, preferred_element_type=jnp.float32)
    return result.astype(jnp.bfloat16).reshape(batches, seq_local, -1)


MESH = pl.DeviceIdType.MESH
HALF = GROUP_WIDTH // 2


def fold_table():
    n = np.arange(GROUP_WIDTH)
    table = np.zeros((2, HALF, GROUP_WIDTH))
    for m in range(HALF):
        table[0, m] = np.cos(2 * np.pi * (n * m % GROUP_WIDTH) / GROUP_WIDTH)
        table[1, m] = np.sin(2 * np.pi * (n * m % GROUP_WIDTH) / GROUP_WIDTH)
    table[1, 0] = np.cos(np.pi * n)
    return table.reshape(GROUP_WIDTH, GROUP_WIDTH)


def first_table(n1):
    a = np.arange(n1)
    ang = 2 * np.pi * (np.outer(a, a) % n1) / n1
    return np.concatenate([np.cos(ang), np.sin(ang)], 0)


def twist_table(n1, n2):
    phi = 2 * np.pi * np.outer(np.arange(n1), np.arange(n2)) / (n1 * n2)
    scale = 1.0 / np.sqrt(n1 * n2 * GROUP_WIDTH)
    return np.stack([np.cos(phi) * scale, np.sin(phi) * scale])


def second_table(rows, n2):
    q = np.arange(n2)
    psi = 2 * np.pi * (np.outer(q, q) % n2) / n2
    cos, sin = np.cos(psi), np.sin(psi)
    even = np.concatenate([cos, sin], 1)
    odd = np.concatenate([sin, -cos], 1)
    zero = np.zeros_like(even)
    plain = np.stack([np.concatenate([even, -odd], 1), np.concatenate([even, odd], 1)])
    first = np.stack([np.concatenate([even, zero], 1), np.concatenate([zero, even], 1)])
    both = np.stack([plain, first])
    per = n2 // rows
    both = both.reshape(2, 2, rows, per, 4 * n2).transpose(0, 3, 2, 1, 4)
    return both.reshape(2, 2 * n2, 4 * n2)


def channel_order(rows, cols):
    take = np.zeros((rows, cols, 2), np.int64)
    for r in range(rows):
        for c in range(cols):
            group = (c + 1 - 2 * (c % 2)) * GROUP_WIDTH
            take[r, c, 0] = group + r
            take[r, c, 1] = group + (HALF if r == 0 else GROUP_WIDTH - r)
    return np.eye(rows * cols * 2)[take.reshape(-1)]


def row_offsets():
    far = lambda n: sorted(range(n), key=lambda d: -min(d, n - d))
    return [(dz, dy) for dy in far(4) for dz in far(8) if dz or dy]


def mixer_kernel(
    rows, cols, tok, gain_in, wf_in, wg_in, wspec_in, wout, fold_in, f1_in, f2_in, tw_in, perm_in, out,
    tokv, gain, wf, wg, wsv, ws, wo, fold, f1, f2, tw, perm, wp, gate, ysc, tt, s1, x1, xs, ps, spec, osc,
    tsem, lsem, s1s, s1r, sws, swr, s2s, s2r, oss, osr, wos, wor, ready,
):
    batches, seq_local, features = tok.shape
    n1, n2 = tw.shape[1:]
    blocks = seq_local // n2
    span = seq_local // cols
    width = wout.shape[1]
    chunk = 512
    chunks = seq_local // chunk
    me = lax.axis_index("row")
    col = lax.axis_index("col")
    z, y = lax.div(me, 4), lax.rem(me, 4)
    sib = col + 1 - 2 * lax.rem(col, 2)
    peers = [lax.rem(z + dz, 8) * 4 + lax.rem(y + dy, 4) for dz, dy in row_offsets()]
    far = [lax.rem(col + 4, cols), lax.rem(sib + 4, cols)]
    near = [lax.rem(col + 2, cols), lax.rem(col + 6, cols), lax.rem(sib + 2, cols), lax.rem(sib + 6, cols)]
    others = far + near + [sib]
    across = [far[1], near[2], near[3]]
    core = lax.rem(col, 2)

    line = [lax.rem(z + dz, 8) * 4 + y for dz, dy in row_offsets() if dy == 0]
    aside = [lax.rem(z + dz, 8) * 4 + lax.rem(y + dy, 4) for dz, dy in row_offsets() if dy]
    turns = [z * 4 + lax.rem(y + d, 4) for d in range(1, 4)]

    def load(src, dst, at):
        copy = pltpu.make_async_copy(src, dst, lsem.at[at])
        copy.start()
        return copy

    def lane_block(c, size):
        return pl.ds(pl.multiple_of(c * size, size), size)

    barrier = pltpu.get_barrier_semaphore()
    for to in line:
        pl.semaphore_signal(
            barrier, inc=1, device_id={"row": to, "col": sib}, device_id_type=MESH
        )
    for to in turns:
        pl.semaphore_signal(barrier, inc=1, device_id={"row": to}, device_id_type=MESH)
    for to in others:
        pl.semaphore_signal(barrier, inc=1, device_id={"col": to}, device_id_type=MESH)

    fold_load = load(fold_in, fold, 0)
    wf_load = load(wf_in, wf, 1)
    gain_load = load(gain_in, gain, 2)
    loads = {}
    for b in range(batches):
        for j in range(chunks):
            part = pl.ds(j * chunk, chunk)
            loads[b, j] = pltpu.make_async_copy(tok.at[b, part], tokv.at[b, part], tsem.at[b, j])
            loads[b, j].start()
    wo_load = load(wout, wo.at[:, lane_block(col, width)], 3)
    wg_load = load(wg_in, wg, 4)
    spec_load = load(wspec_in, wsv, 5)
    perm_load = load(perm_in, perm, 6)
    f1_load = load(f1_in, f1, 7)
    tw_load = load(tw_in, tw, 8)
    f2_load = load(f2_in, f2, 9)

    fold_load.wait()
    wf_load.wait()
    gain_load.wait()
    folded = jnp.zeros((GROUP_WIDTH, features), jnp.float32)
    for half in range(2):
        folded += lax.dot_general(
            fold[half], wf[...], (((1,), (0,)), ((), ())), preferred_element_type=jnp.float32
        )
    wp[...] = (folded * gain[...]).astype(jnp.bfloat16)

    def project(b):
        for j in range(chunks):
            loads[b, j].wait()
            t = tokv[b, j * chunk:(j + 1) * chunk, :]
            part = lax.dot_general(
                wp[...], t, (((1,), (1,)), ((), ())), preferred_element_type=jnp.float32
            )
            squares = jnp.zeros((chunk, LANES), jnp.float32)
            for k in range(features // LANES):
                w = t[:, k * LANES:(k + 1) * LANES].astype(jnp.float32)
                squares += w * w
            total = jnp.sum(squares.T, axis=0, keepdims=True)
            part = part * lax.rsqrt(total * (1.0 / features) + norm_eps)
            for k in range(chunk // n2):
                ysc[pl.ds(j * (chunk // n2) + k, GROUP_WIDTH, stride=blocks), :] = part[:, k * n2:(k + 1) * n2]
        for c in range(2):
            half = ysc[c * rows * blocks:(c + 1) * rows * blocks, :].reshape(rows, blocks, n2)
            s1[b, :, :, c * n2:(c + 1) * n2] = half.astype(jnp.bfloat16)

    def remote(src, dst, send, recv, to):
        return pltpu.make_async_remote_copy(
            src_ref=src, dst_ref=dst, send_sem=send, recv_sem=recv, device_id=to, device_id_type=MESH
        )

    def drain(ref, sem):
        pltpu.make_async_copy(ref, ref, sem).wait()

    def send_first(b, targets):
        for to in targets:
            remote(s1.at[b, to], x1.at[b, me], s1s.at[b], s1r.at[b], {"row": to, "col": sib}).start()

    def gates(b):
        t = tokv[b, pl.ds(pl.multiple_of(col * span, span), span), :].astype(jnp.float32)
        scale = lax.rsqrt(jnp.mean(t * t, axis=-1, keepdims=True) + norm_eps)
        normed = (t * scale * gain[...]).astype(jnp.bfloat16)
        g = jnp.dot(normed, wg[...], preferred_element_type=jnp.float32)
        gate[b] = 0.5 * jnp.tanh(0.5 * g) + 0.5

    def transform(b):
        x = x1[b].reshape(n1, 2 * n2)
        g = jnp.dot(f1[...], x, preferred_element_type=jnp.float32)
        cos, sin = tw[0], tw[1]
        for c in range(2):
            gc = g[:n1, c * n2:(c + 1) * n2]
            gs = g[n1:, c * n2:(c + 1) * n2]
            tt[:, 2 * c * n2:(2 * c + 1) * n2] = (gc * cos - gs * sin).astype(jnp.bfloat16)
            tt[:, (2 * c + 1) * n2:(2 * c + 2) * n2] = (-(gc * sin + gs * cos)).astype(jnp.bfloat16)
        own = jnp.where(me == 0, 1, 0)

        def half(which):
            o = lax.dot_general(
                f2[own], tt[pl.ds(pl.multiple_of(which * span, span), span), :],
                (((1,), (1,)), ((), ())), preferred_element_type=jnp.float32,
            )
            return o.astype(jnp.bfloat16).reshape(rows * cols // 2, 2, span)

        xs[b] = half(core)
        swap(b).start()
        ps[b, :, core] = half(1 - core)

    def swap(b):
        return remote(
            xs.at[b], ps.at[b, :, core], sws.at[b], swr.at[b], {"col": sib}
        )

    def send_second(b):
        def one(to, c):
            remote(
                ps.at[b, lax.div(c, 2) * rows + to], spec.at[b, me, lax.div(col, 2)],
                s2s.at[b], s2r.at[b], {"row": to, "col": c},
            ).start()

        for c in across + [sib]:
            for to in peers + [me]:
                one(to, c)

    def share(owner, at, to):
        part = wo.at[:, lane_block(owner, width)]
        return remote(part, part, wos.at[at], wor.at[at], {"col": to})

    def quarter(owner, at_y, at, to):
        size = wo.shape[0] // 4
        part = wo.at[pl.ds(pl.multiple_of(at_y * size, size), size), lane_block(owner, width)]
        return remote(part, part, wos.at[at], wor.at[at], to)

    def mix(b):
        lhs = spec[b].reshape(2 * rows * cols, span)
        pre = lax.dot_general(
            lhs, ws[...], (((0,), (0,)), ((), ())), preferred_element_type=jnp.float32
        )
        return (gate[b] * pre).astype(jnp.bfloat16)

    def emit(b, mixed):
        for step in range(cols // 2):
            chip = lax.rem(lax.div(col, 2) + (2, 1, 3, 0)[step], cols // 2)
            res = jnp.dot(
                mixed, wo[:, lane_block(chip, 2 * width)], preferred_element_type=jnp.float32
            ).astype(jnp.bfloat16)
            for core in range(2):
                osc[b, chip * 2 + core] = res[:, core * width:(core + 1) * width]
            rest = pl.ds(pl.multiple_of(col * span, span), span)
            targets = (far, near[0::2], near[1::2], [sib])[step]
            for to in targets:
                remote(
                    osc.at[b, to], out.at[b, rest, :], oss.at[b], osr.at[b], {"col": to}
                ).start()
            if step == cols // 2 - 1:
                out[b, rest, :] = osc[b, col]

    scope = jax.named_scope
    with scope("project0"):
        project(0)
    with scope("barrier"):
        pl.semaphore_wait(barrier, len(line) + len(turns) + cols - 1)
    for to in turns:
        pl.semaphore_signal(ready, inc=1, device_id={"row": to}, device_id_type=MESH)
    with scope("send0"):
        send_first(0, line)
    for b in range(1, batches):
        with scope("project%d" % b):
            project(b)
        with scope("line%d" % b):
            send_first(b, line)
    with scope("ready"):
        pl.semaphore_wait(ready, len(turns))
    with scope("send0b"):
        send_first(0, aside + [me])
    wo_load.wait()
    quarter(col, y, 7, {"col": far[0]}).start()
    share(col, 0, near[0]).start()
    share(col, 1, near[1]).start()
    share(col, 3, sib).start()
    with scope("gates"):
        wg_load.wait()
        gates(0)
    with scope("spectrum_rows"):
        spec_load.wait()
        perm_load.wait()
        ws[...] = jnp.dot(
            perm[...], wsv[...], preferred_element_type=jnp.float32
        ).astype(jnp.bfloat16)
        f1_load.wait()
        tw_load.wait()
        f2_load.wait()
    for b in range(1, batches):
        with scope("send%d" % b):
            send_first(b, aside + [me])
        with scope("gates"):
            gates(b)
    with scope("turn"):
        quarter(far[0], y, 7, {"col": sib}).wait_recv()
        for d in (2, 1, 3):
            quarter(far[0], y, 7 + d, {"row": turns[d - 1]}).start()
    for b in range(batches):
        with scope("wait_first%d" % b):
            drain(s1.at[b], s1r.at[b])
        with scope("transform%d" % b):
            transform(b)
        with scope("swap%d" % b):
            swap(b).wait_recv()
        with scope("second%d" % b):
            send_second(b)
        if b == 0:
            with scope("share"):
                share(near[1], 0, sib).wait_recv()
                share(near[1], 4, sib).start()
                share(near[0], 1, sib).wait_recv()
                share(near[0], 5, sib).start()
    with scope("share2"):
        for d in range(1, 4):
            quarter(far[0], y, 7 + d, {"row": turns[d - 1]}).wait_recv()
        share(far[0], 2, sib).start()
        for at in range(2, 6):
            share(col, at, sib).wait_recv()
    for b in range(batches):
        with scope("wait_second%d" % b):
            drain(ps.at[b], s2r.at[b])
        with scope("mix%d" % b):
            mixed = mix(b)
        with scope("emit%d" % b):
            emit(b, mixed)
    with scope("wait_out"):
        for b in range(batches):
            drain(osc.at[b, pl.ds(0, cols - 1)], osr.at[b])
    with scope("tail"):
        for b in range(batches):
            drain(s1.at[b], s1s.at[b])
            drain(ps.at[b], s2s.at[b])
            swap(b).wait_send()
            drain(osc.at[b, pl.ds(0, cols - 1)], oss.at[b])
        for at in range(6):
            share(col, at, sib).wait_send()
        for at in range(7, 11):
            quarter(col, y, at, {"col": sib}).wait_send()


def fused(rows, cols, tokens, norm_gain, w_fourier_in, w_gate, w_spectrum, w_output):
    batches, seq_local, features = tokens.shape
    n2 = LANES
    n1 = seq_local * rows // n2
    blocks = seq_local // n2
    span = seq_local // cols
    width = w_output.shape[1]
    fold = fold_table()
    fold_high = fold.astype(jnp.bfloat16)
    fold_low = (fold - fold_high.astype(np.float64)).astype(jnp.bfloat16)
    tables = (
        jnp.asarray(np.stack([fold_high, fold_low])),
        jnp.asarray(first_table(n1), jnp.bfloat16),
        jnp.asarray(second_table(rows, n2), jnp.bfloat16),
        jnp.asarray(twist_table(n1, n2), jnp.float32),
        jnp.asarray(channel_order(rows, cols), jnp.bfloat16),
    )
    hbm = pl.BlockSpec(memory_space=pltpu.HBM)
    dma = pltpu.SemaphoreType.DMA
    half = jnp.bfloat16
    scratch = [
        (tokens.shape, half), ((1, features), jnp.float32), (w_fourier_in.shape[::-1], half),
        (w_gate.shape, half), (w_spectrum.shape, half), (w_spectrum.shape, half),
        ((features, features), half), *((t.shape, t.dtype) for t in tables),
        ((GROUP_WIDTH, features), half), ((batches, span, features), jnp.float32),
        ((GROUP_WIDTH * blocks, n2), jnp.float32), ((n1, 4 * n2), half),
        ((batches, rows, blocks, 2 * n2), half), ((batches, rows, blocks, 2 * n2), half),
        ((batches, cols // 2 * rows, 2, span), half),
        ((batches, cols // 2 * rows, 2, 2, span), half),
        ((batches, rows, cols // 2, 2, 2, span), half),
        ((batches, cols, span, width), half),
    ]
    return pl.pallas_call(
        functools.partial(mixer_kernel, rows, cols),
        out_shape=pltpu.VMEM((batches, seq_local, width), jnp.bfloat16),
        in_specs=[hbm] * 11,
        out_specs=pl.BlockSpec(memory_space=pltpu.VMEM),
        scratch_shapes=[pltpu.VMEM(shape, dtype) for shape, dtype in scratch] + [
            dma((batches, seq_local // 512)), dma((10,)),
            *(dma((batches,)) for _ in range(8)), dma((11,)), dma((11,)), pltpu.SemaphoreType.REGULAR,
        ],
        compiler_params=pltpu.CompilerParams(
            collective_id=0, has_side_effects=True, vmem_limit_bytes=62 * 1024 * 1024
        ),
    )(tokens, norm_gain[None, :], w_fourier_in.T, w_gate, w_spectrum, w_output, *tables)


def body(rows, cols, *args):
    tokens, w_fourier_in, w_output = args[0], args[2], args[5]
    fits = (
        rows == HALF and cols == 8 and w_fourier_in.shape[1] == GROUP_WIDTH
        and tokens.shape[1:] == (16 * LANES, 8 * LANES) and w_output.shape[1] == LANES
    )
    if fits:
        return fused(rows, cols, *args)
    return on_device(*args)


def solution(mesh):
    placed = (P(None, "row", None), P(), P(None, "col"), P(), P(), P(None, "col"))
    return jax.shard_map(
        functools.partial(body, mesh.shape["row"], mesh.shape["col"]),
        mesh=mesh, in_specs=placed, out_specs=P(None, "row", "col"), check_vma=False,
    )
```
